256 devices in a mesh: ep: 64 (over z, y, core), tp: 4 (over x).
Axes of the slice: x: 4, y: 4, z: 8, core: 2. Of those that a mesh axis runs over, the one named last changes fastest.
Arguments:
- tokens: bfloat16 [1024, 2048], P('ep'), may hold values from -6 to 6
- lengths: int32 [1024], P('ep'), may hold values from 256 to 1023
- cache: bfloat16 [1024, 1024, 512], P('ep', None, 'tp'), may hold values from -6 to 6
- attn_gain: float32 [2048], replicated, may hold values from 0.1 to 1.9
- query_weight: bfloat16 [2048, 1024], P(None, 'tp'), may hold values from -0.125 to 0.125
- key_weight: bfloat16 [2048, 256], P(None, 'tp'), may hold values from -0.125 to 0.125
- value_weight: bfloat16 [2048, 256], P(None, 'tp'), may hold values from -0.125 to 0.125
- stick_bias: float32 [16], P('tp'), may hold values from -7 to -1
- out_weight: bfloat16 [1024, 2048], P('tp'), may hold values from -0.1875 to 0.1875
- ffn_gain: float32 [2048], replicated, may hold values from 0.1 to 1.9
- routes: int32 [1024, 6], P('ep'), may hold values from 0 to 63, all different within a row; in each aligned block of 16 rows (0 to 15, 16 to 31, ...) at most 3 rows name the same one
- route_weights: float32 [1024, 6], P('ep'), may hold values from 0.1 to 0.6
- expert_gate: bfloat16 [64, 2048, 1024], P('ep', None, 'tp'), may hold values from -0.125 to 0.125
- expert_up: bfloat16 [64, 2048, 1024], P('ep', None, 'tp'), may hold values from -0.125 to 0.125
- expert_down: bfloat16 [64, 1024, 2048], P('ep', 'tp'), may hold values from -0.1875 to 0.1875
- shared_gate: bfloat16 [2048, 512], P('ep', 'tp'), may hold values from -0.125 to 0.125
- shared_up: bfloat16 [2048, 512], P('ep', 'tp'), may hold values from -0.125 to 0.125
- shared_down: bfloat16 [512, 2048], P('tp'), may hold values from -0.25 to 0.25
- gate_vector: bfloat16 [2048], replicated, may hold values from -0.125 to 0.125
Outputs:
- layer_out: bfloat16 [1024, 2048], P('ep', 'tp')
- new_kv: bfloat16 [1024, 512], P('ep', 'tp')
The draws below stay inside these ranges and needn't reach their ends.
Inputs may be any that keep to these rules, and one draw needn't show every extreme that they name: Each sequence's new token comes after its lengths cached positions. `routes`: each row names 6 different experts; among the 16 rows of one index of ep no expert is named by more than 3 rows.
All inputs are finite; a program needn't handle non-finite values.
Results may differ from the reference program's by a relative error of at most 0.012.
Values may be sent and summed in bfloat16 or wider, within the bound.
A program may use at most 64 MiB of HBM per device.

```python
import math
import jax
import jax.numpy as jnp
import numpy as np
from jax import lax

D = 2048
HEAD_DIM = 64
Q_HEADS = 16
KV_HEADS = 4
EXPERT_FF = 1024
SHARED_FF = 512
TOP_K = 6
SEQ_DEV = 16
CACHE = 1024
SEQS = 1024
EXPERTS = 64
CAP = 3
N_EP = 64
N_TP = 4


def touch_ends(entries, own_key, low, largest):
    shape = entries.shape
    index_at = [jax.random.randint(jax.random.fold_in(own_key, axis), (), 0, shape[axis]) for axis in range(len(shape))]
    entries = entries.at[tuple(index_at)].set(low)
    longest = shape.index(max(shape))
    index_at[longest] = (index_at[longest] + 1) % shape[longest]
    return entries.at[tuple(index_at)].set(largest)


def steps_of(stream_key, dims, cuts, low, largest):
    def one(axis_at, parts):
        steps = jax.random.uniform(jax.random.fold_in(jax.random.fold_in(stream_key, 6), axis_at), (parts,), jnp.float32, low / len(cuts), largest / len(cuts))
        return jnp.repeat(jnp.exp(steps), dims[axis_at] // parts).reshape((-1,) + (1,) * (len(dims) - axis_at - 1))

    factor_of = one(*cuts[0])
    for cut in cuts[1:]:
        factor_of = factor_of * one(*cut)
    return factor_of


def routed_block(rng, own, number, rows, count, top, bound, lean):
    sequence = jax.random.permutation(rng, count)
    heavy_load, usual = shares(count, rows * top, bound, lean, True), shares(count, rows * top, bound, lean, False)
    places = jnp.arange(count)

    def named(tallies, turn):
        used = int((tallies > 0).sum())
        fixed = max(1, used // 4)
        passed = fixed + (places - fixed + turn * (used - fixed)) % max(1, count - fixed)
        return jnp.zeros((count,), jnp.int32).at[sequence[jnp.where(places < fixed, places, passed)]].set(jnp.asarray(tallies, jnp.int32))

    tallies = jnp.where(number % 4 == 0, named(heavy_load, number // 4), named(usual, number - number // 4 - 1))
    mixed = jax.random.permutation(jax.random.fold_in(own, 3), count)
    source_of, sink = mixed[0:count // 2 * 2:2], mixed[1:count // 2 * 2:2]
    slack = jnp.minimum(tallies[source_of] - 1, bound - tallies[sink]) // 2
    slack = jnp.where((source_of == sequence[0]) | (sink == sequence[0]) | (tallies[sink] == 0), 0, jnp.maximum(slack, 0))
    passed = jax.random.randint(jax.random.fold_in(own, 4), (count // 2,), 0, 1 << 20) % (slack + 1)
    tallies = tallies.at[source_of].add(-passed).at[sink].add(passed)
    items = jnp.searchsorted(jnp.cumsum(tallies), jnp.arange(rows * top), side="right").astype(jnp.int32)
    table = items.reshape(top, rows).T
    table = table[jax.random.permutation(jax.random.fold_in(own, 1), rows)]
    turn = jax.random.randint(jax.random.fold_in(own, 2), (rows, 1), 0, top)
    return jnp.take_along_axis(table, (jnp.arange(top)[None, :] + turn) % top, axis=1)


def shares(count, total, most, skew, full):
    loads = [(1 << 20) // math.isqrt(standing ** skew) + 1 for standing in range(1, count + 1)]
    largest = most if full else min(most, max(-(-total // count), total * loads[0] // sum(loads)))
    least = 1 if total - largest >= count - 1 else 0
    given, surplus = [largest] + [least] * (count - 1), total - largest - least * (count - 1)
    while surplus > 0:
        free = [i for i in range(1, count) if given[i] < largest] or [i for i in range(1, count) if given[i] < most]
        pool, remaining = sum([loads[i] for i in free]), surplus
        for i in free:
            addition = min(most - given[i], max(1, remaining * loads[i] // pool), surplus)
            given[i] = given[i] + addition
            surplus = surplus - addition
    return np.array(given)


def noise(rng, shape, spread, most, shards=(), kind=jnp.bfloat16):
    values = jax.random.normal(rng, shape, jnp.float32) * spread
    if len(shards) > 0:
        values = steps_of(rng, shape, shards, -0.22, 0.18) * values
    return jnp.clip(values, min=-most, max=most).astype(kind)


def setup_inputs(seed: int = 0) -> dict:
    splits = jax.random.split(jax.random.key(seed), 20)
    tokens = noise(splits[0], (SEQS, D), 1.0, 6.0, ((0, 64),))
    lengths = touch_ends(jax.random.randint(splits[1], (SEQS,), CACHE // 4, CACHE), jax.random.fold_in(splits[1], 1), CACHE // 4, CACHE - 1).astype(jnp.int32)
    cache = noise(splits[2], (SEQS, CACHE, 2 * KV_HEADS * HEAD_DIM), 1.0, 6.0, ((0, 64), (2, 4)))
    attn_gain = jnp.clip(1.0 + 0.18 * jax.random.normal(splits[3], (D,), jnp.float32), 0.1, 1.9)
    query_weight = noise(splits[4], (D, Q_HEADS * HEAD_DIM), D ** -0.5, 0.125, ((1, 4),))
    key_weight = noise(splits[5], (D, KV_HEADS * HEAD_DIM), D ** -0.5, 0.125, ((1, 4),))
    value_weight = noise(splits[6], (D, KV_HEADS * HEAD_DIM), D ** -0.5, 0.125, ((1, 4),))
    stick_bias = jnp.clip(-7.0 + 6.0 * jax.random.uniform(splits[7], (Q_HEADS,), jnp.float32) ** steps_of(splits[7], (Q_HEADS,), ((0, 4),), -0.2, 0.2), -7.0, -1.0)
    out_weight = noise(splits[8], (Q_HEADS * HEAD_DIM, D), (Q_HEADS * HEAD_DIM) ** -0.5, 0.1875, ((0, 4),))
    ffn_gain = jnp.clip(1.0 + 0.18 * jax.random.normal(splits[9], (D,), jnp.float32), 0.1, 1.9)
    routes_keys = jax.random.split(jax.random.fold_in(splits[10], 1), SEQS // SEQ_DEV)
    routes_turns = jax.random.permutation(jax.random.fold_in(splits[10], 3), SEQS // SEQ_DEV)
    routes = jax.vmap(lambda own, number: routed_block(jax.random.fold_in(splits[10], 2), own, number, SEQ_DEV, EXPERTS, TOP_K, CAP, 1))(routes_keys, routes_turns).reshape((SEQS, TOP_K))
    route_weights = jnp.clip(0.1 + 0.5 * jax.random.uniform(splits[11], (SEQS, TOP_K), jnp.float32) ** steps_of(splits[11], (SEQS, TOP_K), ((0, 64),), -0.2, 0.2), 0.1, 0.6)
    expert_gate = noise(splits[12], (EXPERTS, D, EXPERT_FF), D ** -0.5, 0.125, ((0, 64), (2, 4)))
    expert_up = noise(splits[13], (EXPERTS, D, EXPERT_FF), D ** -0.5, 0.125, ((0, 64), (2, 4)))
    expert_down = noise(splits[14], (EXPERTS, EXPERT_FF, D), EXPERT_FF ** -0.5, 0.1875, ((0, 64), (1, 4)))
    shared_gate = noise(splits[15], (D, SHARED_FF), D ** -0.5, 0.125, ((0, 64), (1, 4)))
    shared_up = noise(splits[16], (D, SHARED_FF), D ** -0.5, 0.125, ((0, 64), (1, 4)))
    shared_down = noise(splits[17], (SHARED_FF, D), SHARED_FF ** -0.5, 0.25, ((0, 4),))
    gate_vector = noise(splits[18], (D,), D ** -0.5, 0.125)
    return dict(tokens=tokens, lengths=lengths, cache=cache, attn_gain=attn_gain, query_weight=query_weight, key_weight=key_weight, value_weight=value_weight, stick_bias=stick_bias, out_weight=out_weight, ffn_gain=ffn_gain, routes=routes, route_weights=route_weights, expert_gate=expert_gate, expert_up=expert_up, expert_down=expert_down, shared_gate=shared_gate, shared_up=shared_up, shared_down=shared_down, gate_vector=gate_vector)


epsilon = 1e-06

def rms_scale(rows_in, gain_row):
    values_f = rows_in.astype(jnp.float32)
    return values_f * lax.rsqrt(lax.optimization_barrier(jnp.mean(values_f * values_f, axis=-1, keepdims=True)) + epsilon) * gain_row

def block_sum(left_rows, right_rows, blocks):
    row_count, inner = left_rows.shape
    part_width = inner // blocks
    left_view = left_rows.reshape(row_count, blocks, part_width).astype(jnp.float32)
    right_view = right_rows.reshape(blocks, part_width, right_rows.shape[1]).astype(jnp.float32)
    partials = jnp.einsum('nbf,bfd->bnd', left_view, right_view).astype(jnp.bfloat16)
    return lax.optimization_barrier(jnp.sum(partials.astype(jnp.float32), axis=0))

def reference(tokens, lengths, cache, attn_gain, query_weight, key_weight, value_weight, stick_bias, out_weight, ffn_gain, routes, route_weights, expert_gate, expert_up, expert_down, shared_gate, shared_up, shared_down, gate_vector):
    total_rows = tokens.shape[0]
    normed = rms_scale(tokens, attn_gain).astype(jnp.bfloat16)
    queries = jnp.dot(normed, query_weight, preferred_element_type=jnp.float32).astype(jnp.bfloat16)
    key_rows = jnp.dot(normed, key_weight, preferred_element_type=jnp.float32).astype(jnp.bfloat16)
    value_rows = jnp.dot(normed, value_weight, preferred_element_type=jnp.float32).astype(jnp.bfloat16)
    new_kv = jnp.stack([key_rows.reshape(total_rows, KV_HEADS, HEAD_DIM), value_rows.reshape(total_rows, KV_HEADS, HEAD_DIM)], axis=2)
    new_kv = new_kv.reshape(total_rows, 2 * KV_HEADS * HEAD_DIM)
    group_size = Q_HEADS // KV_HEADS
    grouped = queries.reshape(N_EP, SEQ_DEV, KV_HEADS, group_size, HEAD_DIM)
    cache_view = cache.reshape(N_EP, SEQ_DEV, CACHE, KV_HEADS, 2, HEAD_DIM)
    span_rows = lengths.reshape(N_EP, SEQ_DEV)
    offsets = stick_bias.astype(jnp.float32).reshape(1, KV_HEADS, group_size, 1)

    def attend(pieces):
        query_block, cache_block, span_block = pieces
        key_block = cache_block[:, :, :, 0, :].astype(jnp.float32)
        value_block = cache_block[:, :, :, 1, :].astype(jnp.float32)
        scores = jnp.einsum('nkgd,nckd->nkgc', query_block.astype(jnp.float32), key_block) * HEAD_DIM ** (-0.5)
        scores = scores + offsets
        positions = jnp.arange(CACHE, dtype=jnp.int32)
        usable = (positions[None, :] < span_block[:, None])[:, None, None, :]
        log_keep = jnp.where(usable, jax.nn.log_sigmoid(-scores), 0.0)
        behind = lax.cumsum(log_keep, axis=3, reverse=True) - log_keep
        stick_weights = jnp.where(usable, jnp.exp(jax.nn.log_sigmoid(scores) + behind), 0.0).astype(jnp.bfloat16)
        mixed = jnp.einsum('nkgc,nckd->nkgd', stick_weights.astype(jnp.float32), value_block)
        return mixed.astype(jnp.bfloat16)
    heads_out = lax.map(attend, (grouped, cache_view, span_rows)).reshape(total_rows, Q_HEADS * HEAD_DIM)
    residual = tokens.astype(jnp.float32) + block_sum(heads_out, out_weight, N_TP)
    normed_mix = rms_scale(residual, ffn_gain).astype(jnp.bfloat16)
    flat_routes = routes.reshape(-1)
    flat_weights = route_weights.reshape(-1).astype(jnp.float32)
    rows_most = N_EP * CAP

    def run_expert(expert_index):
        routed_here = flat_routes == expert_index
        ordering = jnp.argsort(jnp.where(routed_here, 0, 1).astype(jnp.int32), stable=True)[:rows_most]
        ordering = ordering.astype(jnp.int32)
        owners = (ordering // TOP_K).astype(jnp.int32)
        chosen = normed_mix[owners]
        gate_val = jnp.dot(chosen, expert_gate[expert_index], preferred_element_type=jnp.float32)
        up_val = jnp.dot(chosen, expert_up[expert_index], preferred_element_type=jnp.float32)
        hidden = (jax.nn.silu(gate_val) * up_val).astype(jnp.bfloat16)
        result = block_sum(hidden, expert_down[expert_index], N_TP).astype(jnp.bfloat16)
        route_scale = jnp.where(routed_here[ordering], flat_weights[ordering], 0.0)
        return (owners, result.astype(jnp.float32) * route_scale[:, None])
    owner_rows, contrib = lax.map(run_expert, jnp.arange(EXPERTS, dtype=jnp.int32))
    routed = jnp.zeros((total_rows, D), jnp.float32).at[owner_rows.reshape(-1)].add(contrib.reshape(-1, D))
    shared_gate_val = jnp.dot(normed_mix, shared_gate, preferred_element_type=jnp.float32)
    shared_up_val = jnp.dot(normed_mix, shared_up, preferred_element_type=jnp.float32)
    shared_hidden = (jax.nn.silu(shared_gate_val) * shared_up_val).astype(jnp.bfloat16)
    shared_out = block_sum(shared_hidden, shared_down, N_TP)
    mix_gate = jax.nn.sigmoid(jnp.dot(normed_mix, gate_vector, preferred_element_type=jnp.float32))
    layer_out = (residual + routed + mix_gate[:, None] * shared_out).astype(jnp.bfloat16)
    return (layer_out, new_kv)
```

```python
import functools

import jax
import jax.numpy as jnp
from jax import lax
from jax.experimental import pallas as pl
from jax.experimental.pallas import tpu as pltpu
from jax.sharding import PartitionSpec as P

HEAD_DIM = 64
EPS = 1e-06
CAP = 3
NY = 4
F32 = jnp.float32
BF16 = jnp.bfloat16
MESH = pl.DeviceIdType.MESH
NT = (((1,), (1,)), ((), ()))


def mm(a, b):
    return jnp.dot(a, b, preferred_element_type=F32)


def silu(v):
    return v / (1.0 + jnp.exp(-v))


def kernel(
    dims,
    tokens,
    lengths,
    cache,
    attn_gain,
    query_weight,
    key_weight,
    value_weight,
    stick_bias,
    out_weight,
    ffn_gain,
    routes,
    route_weights,
    expert_gate,
    expert_up,
    expert_down,
    shared_gate,
    shared_up,
    shared_down,
    gate_vector,
    layer_out,
    new_kv,
    tok_v,
    tokq_v,
    again_v,
    fgain_v,
    gv_v,
    routes_v,
    rw_v,
    wq_v,
    wk_v,
    wv_v,
    wo_v,
    eg_v,
    eu_v,
    ed_v,
    sd_v,
    cache_v,
    sgu_v,
    qrow,
    lrow,
    score,
    orow,
    info,
    take,
    comb,
    att,
    att_in,
    res_v,
    res16,
    tb,
    slot_out,
    xs,
    ys,
    ys_in,
    yy,
    ret,
    zs,
    zs_in,
    sh_out,
    sh_in,
    lsem,
    csem,
    info_s,
    info_r,
    sz_s,
    sz_r,
    sy_s,
    sy_r,
    sc_s,
    sc_r,
    at_s,
    at_r,
    rx_s,
    rx_r,
    tz_s,
    tz_r,
    sl_s,
    sl_r,
    xf_s,
    xf_r,
    yx_s,
    yx_r,
    yg_s,
    yg_r,
    sh_s,
    sh_r,
    zb_s,
    zb_r,
):
    nz, ny, nx = dims
    rows, width = tok_v.shape
    quarter = width // nx
    groups = 2 * ny
    part = CAP * nz
    slots = groups * part
    heads = wq_v.shape[1] // HEAD_DIM
    length = cache_v.shape[1]
    ep = lax.axis_index("ep")
    x = lax.axis_index("tp")
    c = ep % 2
    y = (ep // 2) % ny
    z = ep // (2 * ny)

    def device(z_, y_, c_, x_):
        return ((z_ * ny + y_) * 2 + c_, x_)

    def z_peer(d):
        return device((z + d) % nz, y, c, x)

    def g_peer(g):
        return device(z, (y + g // 2) % ny, (c + g % 2) % 2, x)

    def g_back(g):
        return ((ny - g // 2) % ny) * 2 + g % 2

    def x_peer(d):
        return device(z, y, c, (x + d) % nx)

    def remote(src, dst, send, recv, to):
        copy = pltpu.make_async_remote_copy(
            src_ref=src,
            dst_ref=dst,
            send_sem=send,
            recv_sem=recv,
            device_id=to,
            device_id_type=MESH,
        )
        return copy

    peers = (
        [z_peer(d) for d in range(1, nz)]
        + [g_peer(g) for g in range(1, groups)]
        + [x_peer(d) for d in range(1, nx)]
    )
    barrier = pltpu.get_barrier_semaphore()
    for peer in peers:
        pl.semaphore_signal(barrier, inc=1, device_id=peer, device_id_type=MESH)

    local = {}

    def fetch(name, src, dst):
        copy = pltpu.make_async_copy(src, dst, lsem.at[len(local)])
        copy.start()
        local[name] = copy

    own_q = pl.multiple_of(x * quarter, quarter)
    fetch("tok", tokens, tok_v)
    fetch("again", attn_gain, again_v)
    fetch("wq", query_weight, wq_v)
    fetch("wk", key_weight, wk_v)
    fetch("wv", value_weight, wv_v)
    fetch("routes", routes, routes_v)
    fetch("rw", route_weights, rw_v)
    fetch("sg", shared_gate, sgu_v.at[0, z, y, c])
    fetch("su", shared_up, sgu_v.at[1, z, y, c])
    cached = []
    for n in range(rows):
        copy = pltpu.make_async_copy(cache.at[n], cache_v.at[n], csem.at[n])
        copy.start()
        cached.append(copy)
    fetch("wo", out_weight, wo_v)
    fetch("tokq", tokens.at[:, pl.ds(own_q, quarter)], tokq_v)
    fetch("fgain", ffn_gain, fgain_v)
    fetch("gv", gate_vector, gv_v)
    fetch("eg", expert_gate.at[0], eg_v)
    fetch("eu", expert_up.at[0], eu_v)
    fetch("sd", shared_down, sd_v)
    fetch("ed", expert_down.at[0], ed_v)

    local["tok"].wait()
    local["again"].wait()
    tf = tok_v[...].astype(F32)
    normed = (
        tf * lax.rsqrt(jnp.mean(tf * tf, axis=-1, keepdims=True) + EPS) * again_v[...]
    ).astype(BF16)
    local["wq"].wait()
    q = mm(normed, wq_v[...]).astype(BF16).astype(F32)
    local["wk"].wait()
    local["wv"].wait()
    new_kv[...] = jnp.concatenate(
        [mm(normed, wk_v[...]), mm(normed, wv_v[...])], axis=1
    ).astype(BF16)
    for h in range(heads):
        qrow[pl.ds(h, rows, stride=heads), :] = jnp.concatenate(
            [q[:, h * HEAD_DIM : (h + 1) * HEAD_DIM], jnp.zeros((rows, HEAD_DIM), F32)], axis=1
        )
    local["routes"].wait()
    local["rw"].wait()
    top = routes_v.shape[1]
    info[0] = jnp.concatenate(
        [
            routes_v[...].astype(F32),
            rw_v[...],
            jnp.zeros((rows, info.shape[2] - 2 * top), F32),
        ],
        axis=1,
    )

    pl.semaphore_wait(barrier, len(peers))
    local["sg"].wait()
    local["su"].wait()
    sends = []

    def send(*args):
        copy = remote(*args)
        copy.start()
        sends.append(copy)
        return copy

    info_c, sz_c = [], []
    for d in range(1, nz):
        info_c.append(send(info.at[0], info.at[nz - d], info_s.at[d - 1], info_r.at[d - 1], z_peer(d)))
        own = sgu_v.at[:, z, y, c]
        sz_c.append(send(own, own, sz_s.at[d - 1], sz_r.at[d - 1], z_peer(d)))

    for n in range(rows):
        cached[n].wait()
        at = slice(n * heads, (n + 1) * heads)
        score[at, :] = lax.dot_general(
            qrow[at, :].astype(BF16), cache_v[n], NT, preferred_element_type=F32
        )
        lrow[at, :] = jnp.full((heads, 128), lengths[n], jnp.int32)

    block = 256
    table_r = lax.broadcasted_iota(jnp.int32, (block, block), 0)
    table_c = lax.broadcasted_iota(jnp.int32, (block, block), 1)
    later = jnp.where(table_r > table_c, 1.0, 0.0).astype(BF16)
    all_rows = rows * heads
    head_of = lax.broadcasted_iota(jnp.int32, (all_rows, block), 0) & (heads - 1)
    offset = jnp.zeros((all_rows, block), F32)
    for h in range(heads):
        offset = jnp.where(head_of == h, stick_bias[h], offset)
    limit = jnp.concatenate([lrow[...]] * (block // 128), axis=1)
    beyond = jnp.zeros((all_rows, 1), F32)
    for b in reversed(range(length // block)):
        at = slice(b * block, (b + 1) * block)
        zv = score[:, at] * HEAD_DIM ** (-0.5) + offset
        soft = jnp.log1p(jnp.exp(-jnp.abs(zv)))
        usable = (lax.broadcasted_iota(jnp.int32, (all_rows, block), 1) + b * block) < limit
        keep = jnp.where(usable, jnp.minimum(-zv, 0.0) - soft, 0.0)
        high = keep.astype(BF16)
        low = (keep - high.astype(F32)).astype(BF16)
        within = mm(high, later) + mm(low, later)
        score[:, at] = jnp.where(
            usable, jnp.exp(jnp.minimum(zv, 0.0) - soft + within + beyond), 0.0
        )
        beyond = beyond + within[:, 0:1] + keep[:, 0:1]

    for n in range(rows):
        at = slice(n * heads, (n + 1) * heads)
        orow[at, :] = mm(score[at, :].astype(BF16), cache_v[n])
    heads_out = jnp.concatenate(
        [orow[pl.ds(h, rows, stride=heads), :][:, HEAD_DIM : 2 * HEAD_DIM] for h in range(heads)],
        axis=1,
    ).astype(BF16)
    local["wo"].wait()
    for i in range(nx):
        at = slice(i * quarter, (i + 1) * quarter)
        att[i] = mm(heads_out, wo_v[:, at]).astype(BF16)

    at_c = []
    for d in range(1, nx):
        at_c.append(
            send(att.at[(x + d) % nx], att_in.at[d - 1], at_s.at[d - 1], at_r.at[d - 1], x_peer(d))
        )

    for copy in info_c:
        copy.wait_recv()
    many = nz * rows
    lanes = take.shape[0]
    facts = info[...].reshape(many, info.shape[2])
    lane = lax.broadcasted_iota(jnp.int32, (many, lanes), 1).astype(F32)
    tok_id = lax.broadcasted_iota(jnp.int32, (many, lanes), 0).astype(F32)
    l_group = jnp.floor((lane + 0.5) * (1.0 / part))
    in_group = lane - l_group * part
    l_block = jnp.floor((in_group + 0.5) * (1.0 / CAP))
    l_rank = in_group - l_block * CAP
    l_dy = jnp.floor((l_group + 0.25) * 0.5)
    l_y = y.astype(F32) + l_dy
    l_y = jnp.where(l_y >= ny, l_y - ny, l_y)
    l_c = c.astype(F32) + (l_group - 2.0 * l_dy)
    l_c = jnp.where(l_c >= 2.0, l_c - 2.0, l_c)
    l_expert = (z.astype(F32) * ny + l_y) * 2.0 + l_c
    l_expert = jnp.where(lane < slots, l_expert, -1.0)
    hits = jnp.zeros((many, lanes), F32)
    weigh = jnp.zeros((many, lanes), F32)
    for r in range(top):
        same = facts[:, r : r + 1] == l_expert
        hits = jnp.where(same, 1.0, hits)
        weigh = jnp.where(same, facts[:, top + r : top + r + 1], weigh)
    t_block = jnp.floor((tok_id + 0.5) * (1.0 / rows))
    row_t = lax.broadcasted_iota(jnp.int32, (many, many), 0).astype(F32)
    col_t = lax.broadcasted_iota(jnp.int32, (many, many), 1).astype(F32)
    before = jnp.where(
        (jnp.floor((row_t + 0.5) * (1.0 / rows)) == jnp.floor((col_t + 0.5) * (1.0 / rows)))
        & (col_t < row_t),
        1.0,
        0.0,
    ).astype(BF16)
    rank = mm(before, hits.astype(BF16))
    chosen = (hits > 0.5) & (rank == l_rank) & (t_block == l_block)
    take[...] = jnp.where(chosen, 1.0, 0.0).T.astype(BF16)
    weigh = jnp.where(chosen, weigh, 0.0)
    high = weigh.astype(BF16)
    comb[0] = high
    comb[1] = (weigh - high.astype(F32)).astype(BF16)

    for copy in sz_c:
        copy.wait_recv()
    sy_c = []
    for d in range(1, ny):
        col = sgu_v.at[:, :, y, c]
        sy_c.append(send(col, col, sy_s.at[d - 1], sy_r.at[d - 1], g_peer(2 * d)))

    local["tokq"].wait()
    total = tokq_v[...].astype(F32) + att[x].astype(F32)
    for d in range(1, nx):
        at_c[d - 1].wait_recv()
        total = total + att_in[d - 1].astype(F32)
    res_v[...] = total
    rq = total.astype(BF16)
    tb[0] = rq
    res16[x] = rq
    tz_c = []
    for d in range(1, nz):
        tz_c.append(send(tb.at[0], tb.at[nz - d], tz_s.at[d - 1], tz_r.at[d - 1], z_peer(d)))
    rx_c = []
    for d in range(1, nx):
        rx_c.append(send(res16.at[x], res16.at[x], rx_s.at[d - 1], rx_r.at[d - 1], x_peer(d)))

    for copy in tz_c:
        copy.wait_recv()
    picked = mm(take[0:slots, :], tb[...].reshape(many, quarter))
    xs[x, 0] = picked[0:part].astype(BF16)
    sl_c = {}
    for g in range(1, groups):
        slot_out[g - 1] = picked[g * part : (g + 1) * part].astype(BF16)
        sl_c[g_back(g)] = send(
            slot_out.at[g - 1], xs.at[x, g_back(g)], sl_s.at[g - 1], sl_r.at[g - 1], g_peer(g)
        )
    order = [0, 1] + [s for d in range(1, ny) if d != ny // 2 for s in (2 * d, 2 * d + 1)]
    order += [s for s in range(groups) if s not in order]
    xf_c = {}
    for s in order:
        if s:
            sl_c[s].wait_recv()
        for d in range(1, nx):
            xf_c[s, d] = send(
                xs.at[x, s], xs.at[x, s], xf_s.at[s, d - 1], xf_r.at[s, d - 1], x_peer(d)
            )

    for copy in sy_c:
        copy.wait_recv()
    half = sgu_v.at[:, :, :, c]
    sc_c = send(half, half, sc_s.at[0], sc_r.at[0], g_peer(1))

    local["fgain"].wait()
    local["gv"].wait()
    gain = [fgain_v[:, i * quarter : (i + 1) * quarter] for i in range(nx)]
    for copy in rx_c:
        copy.wait_recv()
    mine = [res16[i].astype(F32) for i in range(nx)]
    square = sum(jnp.sum(m * m, axis=-1, keepdims=True) for m in mine)
    scale = lax.rsqrt(square * (1.0 / width) + EPS)
    mix = [(mine[i] * scale * gain[i]).astype(BF16) for i in range(nx)]
    mix_gate = sum(
        jnp.sum(
            mix[i].astype(F32) * gv_v[:, i * quarter : (i + 1) * quarter].astype(F32),
            axis=-1,
            keepdims=True,
        )
        for i in range(nx)
    )
    mix_gate = 1.0 / (1.0 + jnp.exp(-mix_gate))
    sc_c.wait_recv()
    local["sd"].wait()
    joined = jnp.concatenate(mix, axis=1)
    s_width = sgu_v.shape[-1]
    s_gate = mm(joined, sgu_v[0].reshape(width, s_width))
    s_up = mm(joined, sgu_v[1].reshape(width, s_width))
    s_hidden = (silu(s_gate) * s_up).astype(BF16)
    for i in range(nx):
        sh_out[i] = mm(s_hidden, sd_v[:, i * quarter : (i + 1) * quarter]).astype(BF16)
    sh_c = []
    for d in range(1, nx):
        sh_c.append(
            send(sh_out.at[(x + d) % nx], sh_in.at[d - 1], sh_s.at[d - 1], sh_r.at[d - 1], x_peer(d))
        )

    local["eg"].wait()
    local["eu"].wait()
    local["ed"].wait()
    yx_c = {}
    per = groups // 2
    for half_at in range(2):
        some = order[half_at * per : (half_at + 1) * per]
        for s in some:
            for d in range(1, nx):
                xf_c[s, d].wait_recv()
        pieces = [
            jnp.concatenate([xs[i, s].astype(F32) for s in some], axis=0) for i in range(nx)
        ]
        square = sum(jnp.sum(m * m, axis=-1, keepdims=True) for m in pieces)
        scale = lax.rsqrt(square * (1.0 / width) + EPS)
        feats = jnp.concatenate(
            [(pieces[i] * scale * gain[i]).astype(BF16) for i in range(nx)], axis=1
        )
        hidden = (silu(mm(feats, eg_v[...])) * mm(feats, eu_v[...])).astype(BF16)
        for i in range(nx):
            term = mm(hidden, ed_v[:, i * quarter : (i + 1) * quarter])
            for j, s in enumerate(some):
                ys[i, s] = term[j * part : (j + 1) * part].astype(BF16)
        for s in reversed(some):
            for d in range(1, nx):
                yx_c[s, d] = send(
                    ys.at[(x + d) % nx, s],
                    ys_in.at[d - 1, s],
                    yx_s.at[s, d - 1],
                    yx_r.at[s, d - 1],
                    x_peer(d),
                )

    back = [s for h in range(2) for s in reversed(order[h * per : (h + 1) * per])]
    yg_c = {}
    for s in back:
        total = ys[x, s].astype(F32)
        for d in range(1, nx):
            yx_c[s, d].wait_recv()
            total = total + ys_in[d - 1, s].astype(F32)
        if s == 0:
            ret[0] = total.astype(BF16)
        else:
            yy[s - 1] = total.astype(BF16)
            yg_c[g_back(s)] = send(
                yy.at[s - 1], ret.at[g_back(s)], yg_s.at[s - 1], yg_r.at[s - 1], g_peer(s)
            )
    for s in range(1, groups):
        yg_c[s].wait_recv()
    home = jnp.concatenate([ret[g].astype(F32) for g in range(groups)], axis=0).astype(BF16)
    routed = mm(comb[0][:, 0:slots], home) + mm(comb[1][:, 0:slots], home)
    zb_c = []
    for d in range(1, nz):
        zs[d - 1] = routed[d * rows : (d + 1) * rows].astype(BF16)
        zb_c.append(send(zs.at[d - 1], zs_in.at[d - 1], zb_s.at[d - 1], zb_r.at[d - 1], z_peer(d)))

    shared = sh_out[x].astype(F32)
    for d in range(1, nx):
        sh_c[d - 1].wait_recv()
        shared = shared + sh_in[d - 1].astype(F32)
    final = res_v[...] + mix_gate * shared + routed[0:rows]
    for d in range(1, nz):
        zb_c[d - 1].wait_recv()
        final = final + zs_in[d - 1].astype(F32)
    layer_out[...] = final.astype(BF16)
    for copy in sends:
        copy.wait_send()


def shards(nz, ny, *args):
    (
        tokens,
        lengths,
        cache,
        attn_gain,
        query_weight,
        key_weight,
        value_weight,
        stick_bias,
        out_weight,
        ffn_gain,
        routes,
        route_weights,
        expert_gate,
        expert_up,
        expert_down,
        shared_gate,
        shared_up,
        shared_down,
        gate_vector,
    ) = args
    nx = lax.axis_size("tp")
    rows, width = tokens.shape
    quarter = width // nx
    groups = 2 * ny
    part = CAP * nz
    slots = groups * part
    lanes = -(-slots // 128) * 128
    heads = query_weight.shape[1] // HEAD_DIM
    length = cache.shape[1]
    vm = pltpu.VMEM
    dma = pltpu.SemaphoreType.DMA

    def like(a):
        return vm(a.shape, a.dtype)

    attn_gain = attn_gain.reshape(1, width)
    ffn_gain = ffn_gain.reshape(1, width)
    gate_vector = gate_vector.reshape(1, width)
    scratch = [
        like(tokens),
        vm((rows, quarter), BF16),
        like(attn_gain),
        like(ffn_gain),
        like(gate_vector),
        like(routes),
        like(route_weights),
        like(query_weight),
        like(key_weight),
        like(value_weight),
        like(out_weight),
        vm(expert_gate.shape[1:], BF16),
        vm(expert_up.shape[1:], BF16),
        vm(expert_down.shape[1:], BF16),
        like(shared_down),
        like(cache),
        vm((2, nz, ny, 2, *shared_gate.shape), BF16),
        vm((rows * heads, 2 * HEAD_DIM), F32),
        vm((rows * heads, 128), jnp.int32),
        vm((rows * heads, length), F32),
        vm((rows * heads, 2 * HEAD_DIM), F32),
        vm((nz, rows, 128), F32),
        vm((lanes, nz * rows), BF16),
        vm((2, nz * rows, lanes), BF16),
        vm((nx, rows, quarter), BF16),
        vm((nx - 1, rows, quarter), BF16),
        vm((rows, quarter), F32),
        vm((nx, rows, quarter), BF16),
        vm((nz, rows, quarter), BF16),
        vm((groups - 1, part, quarter), BF16),
        vm((nx, groups, part, quarter), BF16),
        vm((nx, groups, part, quarter), BF16),
        vm((nx - 1, groups, part, quarter), BF16),
        vm((groups - 1, part, quarter), BF16),
        vm((groups, part, quarter), BF16),
        vm((nz - 1, rows, quarter), BF16),
        vm((nz - 1, rows, quarter), BF16),
        vm((nx, rows, quarter), BF16),
        vm((nx - 1, rows, quarter), BF16),
        dma((20,)),
        dma((rows,)),
    ]
    for shape in (
        (nz - 1,),
        (nz - 1,),
        (ny - 1,),
        (1,),
        (nx - 1,),
        (nx - 1,),
        (nz - 1,),
        (groups - 1,),
        (groups, nx - 1),
        (groups, nx - 1),
        (groups - 1,),
        (nx - 1,),
        (nz - 1,),
    ):
        scratch += [dma(shape), dma(shape)]
    spaces = [pl.ANY] * 19
    spaces[1] = pltpu.SMEM
    spaces[7] = pltpu.SMEM
    return pl.pallas_call(
        functools.partial(kernel, (nz, ny, nx)),
        out_shape=(
            jax.ShapeDtypeStruct((rows, quarter), BF16),
            jax.ShapeDtypeStruct((rows, 2 * HEAD_DIM), BF16),
        ),
        in_specs=[pl.BlockSpec(memory_space=s) for s in spaces],
        out_specs=(
            pl.BlockSpec(memory_space=pltpu.VMEM),
            pl.BlockSpec(memory_space=pltpu.VMEM),
        ),
        scratch_shapes=scratch,
        compiler_params=pltpu.CompilerParams(
            collective_id=0, has_side_effects=True, vmem_limit_bytes=48 * 1024 * 1024
        ),
    )(
        tokens,
        lengths,
        cache,
        attn_gain,
        query_weight,
        key_weight,
        value_weight,
        stick_bias,
        out_weight,
        ffn_gain,
        routes,
        route_weights,
        expert_gate,
        expert_up,
        expert_down,
        shared_gate,
        shared_up,
        shared_down,
        gate_vector,
    )


def solution(mesh, ny=NY):
    nz = mesh.shape["ep"] // (2 * ny)
    placed = (
        P("ep", None),
        P("ep"),
        P("ep", None, "tp"),
        P(),
        P(None, "tp"),
        P(None, "tp"),
        P(None, "tp"),
        P("tp"),
        P("tp", None),
        P(),
        P("ep", None),
        P("ep", None),
        P("ep", None, "tp"),
        P("ep", None, "tp"),
        P("ep", "tp", None),
        P("ep", "tp"),
        P("ep", "tp"),
        P("tp", None),
        P(),
    )
    return jax.shard_map(
        functools.partial(shards, nz, ny),
        mesh=mesh,
        in_specs=placed,
        out_specs=(P("ep", "tp"), P("ep", "tp")),
        check_vma=False,
    )
```

```python
import functools

import jax
import jax.numpy as jnp
from jax import lax
from jax.experimental import pallas as pl
from jax.experimental.pallas import tpu as pltpu
from jax.sharding import PartitionSpec as P

HEAD_DIM = 64
EPS = 1e-06
CAP = 3
NY = 4
F32 = jnp.float32
BF16 = jnp.bfloat16
MESH = pl.DeviceIdType.MESH
NT = (((1,), (1,)), ((), ()))


def mm(a, b):
    return jnp.dot(a, b, preferred_element_type=F32)


def mm_nt(a, b):
    return lax.dot_general(a, b, NT, preferred_element_type=F32)


def silu(v):
    return v / (1.0 + jnp.exp(-v))


def kernel(
    dims,
    tokens,
    lengths,
    cache,
    attn_gain,
    query_weight,
    key_weight,
    value_weight,
    stick_bias,
    out_weight,
    ffn_gain,
    routes,
    route_weights,
    expert_gate,
    expert_up,
    expert_down,
    shared_gate,
    shared_up,
    shared_down,
    gate_vector,
    layer_out,
    new_kv,
    tok_v,
    tokq_v,
    again_v,
    fgain_v,
    gv_v,
    routes_v,
    rw_v,
    wq_v,
    wk_v,
    wv_v,
    wo_v,
    eg_v,
    eu_v,
    ed_v,
    sd_v,
    cache_v,
    sgu_v,
    qrow,
    lrow,
    score,
    orow,
    info,
    take,
    comb,
    att,
    att_in,
    res_v,
    res16,
    tb,
    slot_out,
    xs,
    ys,
    ys_in,
    yy,
    ret,
    zs,
    zs_in,
    sh_out,
    sh_in,
    lsem,
    csem,
    info_s,
    info_r,
    sz_s,
    sz_r,
    sy_s,
    sy_r,
    sc_s,
    sc_r,
    at_s,
    at_r,
    rx_s,
    rx_r,
    tz_s,
    tz_r,
    sl_s,
    sl_r,
    xf_s,
    xf_r,
    yx_s,
    yx_r,
    yg_s,
    yg_r,
    sh_s,
    sh_r,
    zb_s,
    zb_r,
):
    nz, ny, nx = dims
    rows, width = tok_v.shape
    quarter = width // nx
    groups = 2 * ny
    part = CAP * nz
    slots = groups * part
    heads = wq_v.shape[1] // HEAD_DIM
    length = cache_v.shape[1]
    ep = lax.axis_index("ep")
    x = lax.axis_index("tp")
    c = ep % 2
    y = (ep // 2) % ny
    z = ep // (2 * ny)

    def device(z_, y_, c_, x_):
        return ((z_ * ny + y_) * 2 + c_, x_)

    def z_peer(d):
        return device((z + d) % nz, y, c, x)

    def g_peer(g):
        return device(z, (y + g // 2) % ny, (c + g % 2) % 2, x)

    def g_back(g):
        return ((ny - g // 2) % ny) * 2 + g % 2

    def x_peer(d):
        return device(z, y, c, (x + d) % nx)

    def remote(src, dst, send, recv, to):
        copy = pltpu.make_async_remote_copy(
            src_ref=src,
            dst_ref=dst,
            send_sem=send,
            recv_sem=recv,
            device_id=to,
            device_id_type=MESH,
        )
        return copy

    peers = (
        [z_peer(d) for d in range(1, nz)]
        + [g_peer(g) for g in range(1, groups)]
        + [x_peer(d) for d in range(1, nx)]
    )
    barrier = pltpu.get_barrier_semaphore()
    for peer in peers:
        pl.semaphore_signal(barrier, inc=1, device_id=peer, device_id_type=MESH)

    local = {}

    def fetch(name, src, dst):
        copy = pltpu.make_async_copy(src, dst, lsem.at[len(local)])
        copy.start()
        local[name] = copy

    own_q = pl.multiple_of(x * quarter, quarter)
    fetch("tok", tokens, tok_v)
    fetch("again", attn_gain, again_v)
    fetch("wq", query_weight, wq_v)
    fetch("wk", key_weight, wk_v)
    fetch("wv", value_weight, wv_v)
    fetch("routes", routes, routes_v)
    fetch("rw", route_weights, rw_v)
    fetch("sg", shared_gate, sgu_v.at[0, z, y, c])
    fetch("su", shared_up, sgu_v.at[1, z, y, c])
    cached = []
    for n in range(rows):
        copy = pltpu.make_async_copy(cache.at[n], cache_v.at[n], csem.at[n])
        copy.start()
        cached.append(copy)
    fetch("wo", out_weight, wo_v)
    fetch("tokq", tokens.at[:, pl.ds(own_q, quarter)], tokq_v)
    fetch("fgain", ffn_gain, fgain_v)
    fetch("gv", gate_vector, gv_v)
    fetch("eg", expert_gate.at[0], eg_v)
    fetch("eu", expert_up.at[0], eu_v)
    fetch("sd", shared_down, sd_v)
    fetch("ed", expert_down.at[0], ed_v)

    local["tok"].wait()
    local["again"].wait()
    tf = tok_v[...].astype(F32)
    normed = (
        tf * lax.rsqrt(jnp.mean(tf * tf, axis=-1, keepdims=True) + EPS) * again_v[...]
    ).astype(BF16)
    local["wq"].wait()
    q = mm(normed, wq_v[...]).astype(BF16).astype(F32)
    local["wk"].wait()
    local["wv"].wait()
    new_kv[...] = jnp.concatenate(
        [mm_nt(normed, wk_v[...]), mm_nt(normed, wv_v[...])], axis=1
    ).astype(BF16)
    for h in range(heads):
        qrow[pl.ds(h, rows, stride=heads), :] = jnp.concatenate(
            [q[:, h * HEAD_DIM : (h + 1) * HEAD_DIM], jnp.zeros((rows, HEAD_DIM), F32)], axis=1
        )
    local["routes"].wait()
    local["rw"].wait()
    top = routes_v.shape[0]
    named = jnp.concatenate(
        [
            jnp.concatenate([routes_v[...].astype(F32), jnp.zeros((8 - top, rows), F32)], axis=0),
            jnp.concatenate([rw_v[...], jnp.zeros((8 - top, rows), F32)], axis=0),
        ],
        axis=0,
    )
    named = jnp.concatenate([named, jnp.zeros((16, 128 - rows), F32)], axis=1)
    named = jnp.concatenate([named, jnp.zeros((112, 128), F32)], axis=0)
    info[0] = named.T[0:rows]

    pl.semaphore_wait(barrier, len(peers))
    local["sg"].wait()
    local["su"].wait()
    sends = []

    def send(*args):
        copy = remote(*args)
        copy.start()
        sends.append(copy)
        return copy

    info_c, sz_c = [], []
    for d in range(1, nz):
        info_c.append(send(info.at[0], info.at[nz - d], info_s.at[d - 1], info_r.at[d - 1], z_peer(d)))
        own = sgu_v.at[:, z, y, c]
        sz_c.append(send(own, own, sz_s.at[d - 1], sz_r.at[d - 1], z_peer(d)))

    for n in range(rows):
        cached[n].wait()
        at = slice(n * heads, (n + 1) * heads)
        score[at, :] = mm_nt(qrow[at, :].astype(BF16), cache_v[n])
        lrow[at, :] = jnp.full((heads, 128), lengths[n], jnp.int32)

    block = 256
    table_r = lax.broadcasted_iota(jnp.int32, (block, block), 0)
    table_c = lax.broadcasted_iota(jnp.int32, (block, block), 1)
    later = jnp.where(table_r > table_c, 1.0, 0.0).astype(BF16)
    all_rows = rows * heads
    head_of = lax.broadcasted_iota(jnp.int32, (all_rows, block), 0) & (heads - 1)
    offset = jnp.zeros((all_rows, block), F32)
    for h in range(heads):
        offset = jnp.where(head_of == h, stick_bias[h], offset)
    limit = jnp.concatenate([lrow[...]] * (block // 128), axis=1)
    beyond = jnp.zeros((all_rows, 1), F32)
    for b in reversed(range(length // block)):
        at = slice(b * block, (b + 1) * block)
        zv = score[:, at] * HEAD_DIM ** (-0.5) + offset
        soft = jnp.log1p(jnp.exp(-jnp.abs(zv)))
        usable = (lax.broadcasted_iota(jnp.int32, (all_rows, block), 1) + b * block) < limit
        keep = jnp.where(usable, jnp.minimum(-zv, 0.0) - soft, 0.0)
        high = keep.astype(BF16)
        low = (keep - high.astype(F32)).astype(BF16)
        within = mm(high, later) + mm(low, later)
        score[:, at] = jnp.where(
            usable, jnp.exp(jnp.minimum(zv, 0.0) - soft + within + beyond), 0.0
        )
        beyond = beyond + within[:, 0:1] + keep[:, 0:1]

    for n in range(rows):
        at = slice(n * heads, (n + 1) * heads)
        orow[at, :] = mm(score[at, :].astype(BF16), cache_v[n])
    heads_out = jnp.concatenate(
        [orow[pl.ds(h, rows, stride=heads), :][:, HEAD_DIM : 2 * HEAD_DIM] for h in range(heads)],
        axis=1,
    ).astype(BF16)
    local["wo"].wait()
    for i in range(nx):
        at = slice(i * quarter, (i + 1) * quarter)
        att[i] = mm(heads_out, wo_v[:, at]).astype(BF16)

    at_c = []
    for d in range(1, nx):
        at_c.append(
            send(att.at[(x + d) % nx], att_in.at[d - 1], at_s.at[d - 1], at_r.at[d - 1], x_peer(d))
        )

    for copy in info_c:
        copy.wait_recv()
    many = nz * rows
    lanes = take.shape[0]
    facts = info[...].reshape(many, info.shape[2])
    lane = lax.broadcasted_iota(jnp.int32, (many, lanes), 1).astype(F32)
    tok_id = lax.broadcasted_iota(jnp.int32, (many, lanes), 0).astype(F32)
    l_group = jnp.floor((lane + 0.5) * (1.0 / part))
    in_group = lane - l_group * part
    l_block = jnp.floor((in_group + 0.5) * (1.0 / CAP))
    l_rank = in_group - l_block * CAP
    l_dy = jnp.floor((l_group + 0.25) * 0.5)
    l_y = y.astype(F32) + l_dy
    l_y = jnp.where(l_y >= ny, l_y - ny, l_y)
    l_c = c.astype(F32) + (l_group - 2.0 * l_dy)
    l_c = jnp.where(l_c >= 2.0, l_c - 2.0, l_c)
    l_expert = (z.astype(F32) * ny + l_y) * 2.0 + l_c
    l_expert = jnp.where(lane < slots, l_expert, -1.0)
    hits = jnp.zeros((many, lanes), F32)
    weigh = jnp.zeros((many, lanes), F32)
    for r in range(top):
        same = facts[:, r : r + 1] == l_expert
        hits = jnp.where(same, 1.0, hits)
        weigh = jnp.where(same, facts[:, 8 + r : 9 + r], weigh)
    t_block = jnp.floor((tok_id + 0.5) * (1.0 / rows))
    row_t = lax.broadcasted_iota(jnp.int32, (many, many), 0).astype(F32)
    col_t = lax.broadcasted_iota(jnp.int32, (many, many), 1).astype(F32)
    before = jnp.where(
        (jnp.floor((row_t + 0.5) * (1.0 / rows)) == jnp.floor((col_t + 0.5) * (1.0 / rows)))
        & (col_t < row_t),
        1.0,
        0.0,
    ).astype(BF16)
    rank = mm(before, hits.astype(BF16))
    chosen = (hits > 0.5) & (rank == l_rank) & (t_block == l_block)
    take[...] = jnp.where(chosen, 1.0, 0.0).T.astype(BF16)
    weigh = jnp.where(chosen, weigh, 0.0)
    high = weigh.astype(BF16)
    comb[0] = high
    comb[1] = (weigh - high.astype(F32)).astype(BF16)

    for copy in sz_c:
        copy.wait_recv()
    sy_c = []
    for d in range(1, ny):
        col = sgu_v.at[:, :, y, c]
        sy_c.append(send(col, col, sy_s.at[d - 1], sy_r.at[d - 1], g_peer(2 * d)))

    local["tokq"].wait()
    total = tokq_v[...].astype(F32) + att[x].astype(F32)
    for d in range(1, nx):
        at_c[d - 1].wait_recv()
        total = total + att_in[d - 1].astype(F32)
    res_v[...] = total
    rq = total.astype(BF16)
    tb[0] = rq
    res16[x] = rq
    tz_c = []
    for d in range(1, nz):
        tz_c.append(send(tb.at[0], tb.at[nz - d], tz_s.at[d - 1], tz_r.at[d - 1], z_peer(d)))
    rx_c = []
    for d in range(1, nx):
        rx_c.append(send(res16.at[x], res16.at[x], rx_s.at[d - 1], rx_r.at[d - 1], x_peer(d)))

    for copy in tz_c:
        copy.wait_recv()
    picked = mm(take[0:slots, :], tb[...].reshape(many, quarter))
    xs[x, 0] = picked[0:part].astype(BF16)
    sl_c = {}
    for g in range(1, groups):
        slot_out[g - 1] = picked[g * part : (g + 1) * part].astype(BF16)
        sl_c[g_back(g)] = send(
            slot_out.at[g - 1], xs.at[x, g_back(g)], sl_s.at[g - 1], sl_r.at[g - 1], g_peer(g)
        )
    order = [0, 1] + [s for d in range(1, ny) if d != ny // 2 for s in (2 * d, 2 * d + 1)]
    order += [s for s in range(groups) if s not in order]
    xf_c = {}
    for s in order:
        if s:
            sl_c[s].wait_recv()
        for d in range(1, nx):
            xf_c[s, d] = send(
                xs.at[x, s], xs.at[x, s], xf_s.at[s, d - 1], xf_r.at[s, d - 1], x_peer(d)
            )

    for copy in sy_c:
        copy.wait_recv()
    half = sgu_v.at[:, :, :, c]
    sc_c = send(half, half, sc_s.at[0], sc_r.at[0], g_peer(1))

    local["fgain"].wait()
    local["gv"].wait()
    gain = [fgain_v[:, i * quarter : (i + 1) * quarter] for i in range(nx)]
    for copy in rx_c:
        copy.wait_recv()
    mine = [res16[i].astype(F32) for i in range(nx)]
    square = sum(jnp.sum(m * m, axis=-1, keepdims=True) for m in mine)
    scale = lax.rsqrt(square * (1.0 / width) + EPS)
    mix = [(mine[i] * scale * gain[i]).astype(BF16) for i in range(nx)]
    joined = jnp.concatenate(mix, axis=1)
    gv = gv_v[...].astype(F32)
    mix_gate = sum(
        joined[:, i * 128 : (i + 1) * 128].astype(F32) * gv[i : i + 1] for i in range(width // 128)
    )
    mix_gate = jnp.sum(mix_gate, axis=-1, keepdims=True)
    mix_gate = 1.0 / (1.0 + jnp.exp(-mix_gate))
    sc_c.wait_recv()
    local["sd"].wait()
    s_width = sgu_v.shape[-1]
    s_gate = mm(joined, sgu_v[0].reshape(width, s_width))
    s_up = mm(joined, sgu_v[1].reshape(width, s_width))
    s_hidden = (silu(s_gate) * s_up).astype(BF16)
    for i in range(nx):
        sh_out[i] = mm(s_hidden, sd_v[:, i * quarter : (i + 1) * quarter]).astype(BF16)
    sh_c = []
    for d in range(1, nx):
        sh_c.append(
            send(sh_out.at[(x + d) % nx], sh_in.at[d - 1], sh_s.at[d - 1], sh_r.at[d - 1], x_peer(d))
        )

    local["eg"].wait()
    local["eu"].wait()
    local["ed"].wait()
    yx_c = {}
    per = groups // 2
    for half_at in range(2):
        some = order[half_at * per : (half_at + 1) * per]
        for s in some:
            for d in range(1, nx):
                xf_c[s, d].wait_recv()
        pieces = [
            jnp.concatenate([xs[i, s].astype(F32) for s in some], axis=0) for i in range(nx)
        ]
        square = sum(jnp.sum(m * m, axis=-1, keepdims=True) for m in pieces)
        scale = lax.rsqrt(square * (1.0 / width) + EPS)
        feats = jnp.concatenate(
            [(pieces[i] * scale * gain[i]).astype(BF16) for i in range(nx)], axis=1
        )
        hidden = (silu(mm(feats, eg_v[...])) * mm(feats, eu_v[...])).astype(BF16)
        for i in range(nx):
            term = mm(hidden, ed_v[:, i * quarter : (i + 1) * quarter])
            for j, s in enumerate(some):
                ys[i, s] = term[j * part : (j + 1) * part].astype(BF16)
        for s in reversed(some):
            for d in range(1, nx):
                yx_c[s, d] = send(
                    ys.at[(x + d) % nx, s],
                    ys_in.at[d - 1, s],
                    yx_s.at[s, d - 1],
                    yx_r.at[s, d - 1],
                    x_peer(d),
                )

    back = [s for h in range(2) for s in reversed(order[h * per : (h + 1) * per])]
    yg_c = {}
    for s in back:
        total = ys[x, s].astype(F32)
        for d in range(1, nx):
            yx_c[s, d].wait_recv()
            total = total + ys_in[d - 1, s].astype(F32)
        if s == 0:
            ret[0] = total.astype(BF16)
        else:
            yy[s - 1] = total.astype(BF16)
            yg_c[g_back(s)] = send(
                yy.at[s - 1], ret.at[g_back(s)], yg_s.at[s - 1], yg_r.at[s - 1], g_peer(s)
            )
    for s in range(1, groups):
        yg_c[s].wait_recv()
    home = jnp.concatenate([ret[g].astype(F32) for g in range(groups)], axis=0).astype(BF16)
    routed = mm(comb[0][:, 0:slots], home) + mm(comb[1][:, 0:slots], home)
    zb_c = []
    for d in range(1, nz):
        zs[d - 1] = routed[d * rows : (d + 1) * rows].astype(BF16)
        zb_c.append(send(zs.at[d - 1], zs_in.at[d - 1], zb_s.at[d - 1], zb_r.at[d - 1], z_peer(d)))

    shared = sh_out[x].astype(F32)
    for d in range(1, nx):
        sh_c[d - 1].wait_recv()
        shared = shared + sh_in[d - 1].astype(F32)
    final = res_v[...] + mix_gate * shared + routed[0:rows]
    for d in range(1, nz):
        zb_c[d - 1].wait_recv()
        final = final + zs_in[d - 1].astype(F32)
    layer_out[...] = final.astype(BF16)
    for copy in sends:
        copy.wait_send()


def shards(nz, ny, *args):
    (
        tokens,
        lengths,
        cache,
        attn_gain,
        query_weight,
        key_weight,
        value_weight,
        stick_bias,
        out_weight,
        ffn_gain,
        routes,
        route_weights,
        expert_gate,
        expert_up,
        expert_down,
        shared_gate,
        shared_up,
        shared_down,
        gate_vector,
    ) = args
    nx = lax.axis_size("tp")
    rows, width = tokens.shape
    quarter = width // nx
    groups = 2 * ny
    part = CAP * nz
    slots = groups * part
    lanes = -(-slots // 128) * 128
    heads = query_weight.shape[1] // HEAD_DIM
    length = cache.shape[1]
    vm = pltpu.VMEM
    dma = pltpu.SemaphoreType.DMA

    def like(a):
        return vm(a.shape, a.dtype)

    key_weight, value_weight = key_weight.T, value_weight.T
    routes, route_weights = routes.T, route_weights.T
    attn_gain = attn_gain.reshape(1, width)
    ffn_gain = ffn_gain.reshape(1, width)
    gate_vector = gate_vector.reshape(width // 128, 128)
    scratch = [
        like(tokens),
        vm((rows, quarter), BF16),
        like(attn_gain),
        like(ffn_gain),
        like(gate_vector),
        like(routes),
        like(route_weights),
        like(query_weight),
        like(key_weight),
        like(value_weight),
        like(out_weight),
        vm(expert_gate.shape[1:], BF16),
        vm(expert_up.shape[1:], BF16),
        vm(expert_down.shape[1:], BF16),
        like(shared_down),
        like(cache),
        vm((2, nz, ny, 2, *shared_gate.shape), BF16),
        vm((rows * heads, 2 * HEAD_DIM), F32),
        vm((rows * heads, 128), jnp.int32),
        vm((rows * heads, length), F32),
        vm((rows * heads, 2 * HEAD_DIM), F32),
        vm((nz, rows, 128), F32),
        vm((lanes, nz * rows), BF16),
        vm((2, nz * rows, lanes), BF16),
        vm((nx, rows, quarter), BF16),
        vm((nx - 1, rows, quarter), BF16),
        vm((rows, quarter), F32),
        vm((nx, rows, quarter), BF16),
        vm((nz, rows, quarter), BF16),
        vm((groups - 1, part, quarter), BF16),
        vm((nx, groups, part, quarter), BF16),
        vm((nx, groups, part, quarter), BF16),
        vm((nx - 1, groups, part, quarter), BF16),
        vm((groups - 1, part, quarter), BF16),
        vm((groups, part, quarter), BF16),
        vm((nz - 1, rows, quarter), BF16),
        vm((nz - 1, rows, quarter), BF16),
        vm((nx, rows, quarter), BF16),
        vm((nx - 1, rows, quarter), BF16),
        dma((20,)),
        dma((rows,)),
    ]
    for shape in (
        (nz - 1,),
        (nz - 1,),
        (ny - 1,),
        (1,),
        (nx - 1,),
        (nx - 1,),
        (nz - 1,),
        (groups - 1,),
        (groups, nx - 1),
        (groups, nx - 1),
        (groups - 1,),
        (nx - 1,),
        (nz - 1,),
    ):
        scratch += [dma(shape), dma(shape)]
    spaces = [pl.ANY] * 19
    spaces[1] = pltpu.SMEM
    spaces[7] = pltpu.SMEM
    return pl.pallas_call(
        functools.partial(kernel, (nz, ny, nx)),
        out_shape=(
            jax.ShapeDtypeStruct((rows, quarter), BF16),
            jax.ShapeDtypeStruct((rows, 2 * HEAD_DIM), BF16),
        ),
        in_specs=[pl.BlockSpec(memory_space=s) for s in spaces],
        out_specs=(
            pl.BlockSpec(memory_space=pltpu.VMEM),
            pl.BlockSpec(memory_space=pltpu.VMEM),
        ),
        scratch_shapes=scratch,
        compiler_params=pltpu.CompilerParams(
            collective_id=0, has_side_effects=True, vmem_limit_bytes=67043328
        ),
    )(
        tokens,
        lengths,
        cache,
        attn_gain,
        query_weight,
        key_weight,
        value_weight,
        stick_bias,
        out_weight,
        ffn_gain,
        routes,
        route_weights,
        expert_gate,
        expert_up,
        expert_down,
        shared_gate,
        shared_up,
        shared_down,
        gate_vector,
    )


def solution(mesh, ny=NY):
    nz = mesh.shape["ep"] // (2 * ny)
    placed = (
        P("ep", None),
        P("ep"),
        P("ep", None, "tp"),
        P(),
        P(None, "tp"),
        P(None, "tp"),
        P(None, "tp"),
        P("tp"),
        P("tp", None),
        P(),
        P("ep", None),
        P("ep", None),
        P("ep", None, "tp"),
        P("ep", None, "tp"),
        P("ep", "tp", None),
        P("ep", "tp"),
        P("ep", "tp"),
        P("tp", None),
        P(),
    )
    return jax.shard_map(
        functools.partial(shards, nz, ny),
        mesh=mesh,
        in_specs=placed,
        out_specs=(P("ep", "tp"), P("ep", "tp")),
        check_vma=False,
    )
```

```python
import functools

import jax
import jax.numpy as jnp
from jax import lax
from jax.experimental import pallas as pl
from jax.experimental.pallas import tpu as pltpu
from jax.sharding import PartitionSpec as P

HEAD_DIM = 64
EPS = 1e-06
CAP = 3
NY = 4
RIGHT = (0, 1, 2, 4, 5)
F32 = jnp.float32
BF16 = jnp.bfloat16
MESH = pl.DeviceIdType.MESH
NT = (((1,), (1,)), ((), ()))


def mm(a, b):
    return jnp.dot(a, b, preferred_element_type=F32)


def mm_nt(a, b):
    return lax.dot_general(a, b, NT, preferred_element_type=F32)


def silu(v):
    return v / (1.0 + jnp.exp(-v))


def kernel(
    dims,
    tokens,
    lengths,
    cache,
    attn_gain,
    query_weight,
    key_weight,
    value_weight,
    stick_bias,
    out_weight,
    ffn_gain,
    routes,
    route_weights,
    expert_gate,
    expert_up,
    expert_down,
    shared_gate,
    shared_up,
    shared_down,
    gate_vector,
    layer_out,
    new_kv,
    len_m,
    bias_m,
    tok_v,
    tokq_v,
    again_v,
    fgain_v,
    gv_v,
    routes_v,
    rw_v,
    wq_v,
    wk_v,
    wv_v,
    wo_v,
    eg_v,
    eu_v,
    ed_v,
    sd_v,
    cache_v,
    sgu_v,
    qrow,
    lrow,
    score,
    orow,
    info,
    take,
    comb,
    att,
    att_in,
    res_v,
    res16,
    tb,
    slot_out,
    xs,
    ys,
    ys_in,
    opp_in,
    opp_out,
    yy,
    ret,
    zs,
    zs_in,
    sh_out,
    sh_in,
    lsem,
    csem,
    out_s,
    in_r,
    sl_r,
    xf_r,
    yo_r,
    yn_r,
    xc_r,
):
    nz, ny, nx = dims
    rows, width = tok_v.shape
    quarter = width // nx
    groups = 2 * ny
    part = CAP * nz
    slots = groups * part
    heads = wq_v.shape[1] // HEAD_DIM
    length = cache_v.shape[1]
    ep = lax.axis_index("ep")
    x = lax.axis_index("tp")
    c = ep % 2
    y = (ep // 2) % ny
    z = ep // (2 * ny)

    def device(z_, y_, c_, x_):
        return ((z_ * ny + y_) * 2 + c_, x_)

    def z_peer(d):
        return device((z + d) % nz, y, c, x)

    def g_peer(g):
        return device(z, (y + g // 2) % ny, (c + g % 2) % 2, x)

    def g_back(g):
        return ((ny - g // 2) % ny) * 2 + g % 2

    def x_peer(d):
        return device(z, y, c, (x + d) % nx)

    def remote(src, dst, send, recv, to):
        copy = pltpu.make_async_remote_copy(
            src_ref=src,
            dst_ref=dst,
            send_sem=send,
            recv_sem=recv,
            device_id=to,
            device_id_type=MESH,
        )
        return copy

    peers = (
        [z_peer(d) for d in range(1, nz)]
        + [g_peer(g) for g in range(1, groups)]
        + [x_peer(d) for d in range(1, nx)]
    )
    barrier = pltpu.get_barrier_semaphore()
    for peer in peers:
        pl.semaphore_signal(barrier, inc=1, device_id=peer, device_id_type=MESH)

    local = {}

    def fetch(name, src, dst):
        copy = pltpu.make_async_copy(src, dst, lsem.at[len(local)])
        copy.start()
        local[name] = copy

    own_q = pl.multiple_of(x * quarter, quarter)
    fetch("tok", tokens, tok_v)
    fetch("again", attn_gain, again_v)
    fetch("wq", query_weight, wq_v)
    fetch("wk", key_weight, wk_v)
    fetch("wv", value_weight, wv_v)
    fetch("routes", routes, routes_v)
    fetch("rw", route_weights, rw_v)
    fetch("len", lengths, len_m)
    fetch("bias", stick_bias, bias_m)
    fetch("sg", shared_gate, sgu_v.at[0, z, y, c])
    fetch("su", shared_up, sgu_v.at[1, z, y, c])
    chunk = rows // 4
    cached = []
    for n in range(4):
        at = pl.ds(n * chunk, chunk)
        copy = pltpu.make_async_copy(cache.at[at], cache_v.at[at], csem.at[n])
        copy.start()
        cached.append(copy)
    fetch("wo", out_weight, wo_v)
    fetch("tokq", tokens.at[:, pl.ds(own_q, quarter)], tokq_v)
    fetch("fgain", ffn_gain, fgain_v)
    fetch("gv", gate_vector, gv_v)
    fetch("eg", expert_gate.at[0], eg_v)
    fetch("eu", expert_up.at[0], eu_v)
    fetch("sd", shared_down, sd_v)
    fetch("ed", expert_down.at[0], ed_v)

    local["tok"].wait()
    local["again"].wait()
    tf = tok_v[...].astype(F32)
    normed = (
        tf * lax.rsqrt(jnp.mean(tf * tf, axis=-1, keepdims=True) + EPS) * again_v[...]
    ).astype(BF16)
    local["wq"].wait()
    q = mm(normed, wq_v[...]).astype(BF16).astype(F32)
    local["wk"].wait()
    local["wv"].wait()
    new_kv[...] = jnp.concatenate(
        [mm_nt(normed, wk_v[...]), mm_nt(normed, wv_v[...])], axis=1
    ).astype(BF16)
    for h in range(heads):
        qrow[pl.ds(h, rows, stride=heads), :] = jnp.concatenate(
            [q[:, h * HEAD_DIM : (h + 1) * HEAD_DIM], jnp.zeros((rows, HEAD_DIM), F32)], axis=1
        )
    local["routes"].wait()
    local["rw"].wait()
    top = routes_v.shape[0]
    info[0] = jnp.concatenate(
        [
            jnp.concatenate(
                [routes_v[...].astype(F32), rw_v[...], jnp.zeros((top, 128 - 2 * rows), F32)], axis=1
            ),
            jnp.zeros((8 - top, 128), F32),
        ],
        axis=0,
    )

    pl.semaphore_wait(barrier, len(peers))
    local["sg"].wait()
    local["su"].wait()
    INFO, SZ, SY, SC, AT, RX, TZ, SL, XF, YX, YG, SH, ZB = range(13)
    LAST = SL
    posted = {}

    def send(step, src, dst, recv, to, total):
        posted[step] = total
        remote(src, dst, out_s.at[step], recv, to).start()

    def arrived(ref, sem):
        pltpu.make_async_copy(ref, ref, sem).wait()

    far_z = sorted(range(1, nz), key=lambda d: -min(d, nz - d))
    far_y = sorted(range(1, ny), key=lambda d: -min(d, ny - d))
    far_x = sorted(range(1, nx), key=lambda d: -min(d, nx - d))
    others = info.at[pl.ds(1, nz - 1)]
    columns = sgu_v.at[:, pl.ds(0, nz - 1), 0, 0]
    own = sgu_v.at[:, z, y, c]
    for d in far_z:
        send(SZ, own, own, in_r.at[SZ], z_peer(d), columns)
    for d in far_z:
        send(INFO, info.at[0], info.at[nz - d], in_r.at[INFO], z_peer(d), others)

    local["len"].wait()
    local["bias"].wait()
    for n in range(rows):
        if n % chunk == 0:
            cached[n // chunk].wait()
        at = slice(n * heads, (n + 1) * heads)
        score[at, :] = mm_nt(qrow[at, :].astype(BF16), cache_v[n])
        lrow[at, :] = jnp.full((heads, 128), len_m[n], jnp.int32)

    block = 256
    table_r = lax.broadcasted_iota(jnp.int32, (block, block), 0)
    table_c = lax.broadcasted_iota(jnp.int32, (block, block), 1)
    later = jnp.where(table_r > table_c, 1.0, 0.0).astype(BF16)
    all_rows = rows * heads
    head_of = lax.broadcasted_iota(jnp.int32, (all_rows, block), 0) & (heads - 1)
    offset = jnp.zeros((all_rows, block), F32)
    for h in range(heads):
        offset = jnp.where(head_of == h, bias_m[h], offset)
    limit = jnp.concatenate([lrow[...]] * (block // 128), axis=1)
    beyond = jnp.zeros((all_rows, 1), F32)
    for b in reversed(range(length // block)):
        at = slice(b * block, (b + 1) * block)
        zv = score[:, at] * HEAD_DIM ** (-0.5) + offset
        soft = jnp.log1p(jnp.exp(-jnp.abs(zv)))
        usable = (lax.broadcasted_iota(jnp.int32, (all_rows, block), 1) + b * block) < limit
        keep = jnp.where(usable, jnp.minimum(-zv, 0.0) - soft, 0.0)
        high = keep.astype(BF16)
        low = (keep - high.astype(F32)).astype(BF16)
        within = mm(high, later) + mm(low, later)
        score[:, at] = jnp.where(
            usable, jnp.exp(jnp.minimum(zv, 0.0) - soft + within + beyond), 0.0
        )
        beyond = beyond + within[:, 0:1] + keep[:, 0:1]

    for n in range(rows):
        at = slice(n * heads, (n + 1) * heads)
        orow[at, :] = mm(score[at, :].astype(BF16), cache_v[n])
    heads_out = jnp.concatenate(
        [orow[pl.ds(h, rows, stride=heads), :][:, HEAD_DIM : 2 * HEAD_DIM] for h in range(heads)],
        axis=1,
    ).astype(BF16)
    local["wo"].wait()
    for i in range(nx):
        at = slice(i * quarter, (i + 1) * quarter)
        att[i] = mm(heads_out, wo_v[:, at]).astype(BF16)

    for d in far_x:
        send(AT, att.at[(x + d) % nx], att_in.at[d - 1], in_r.at[AT], x_peer(d), att_in)

    local["tokq"].wait()
    total = tokq_v[...].astype(F32) + att[x].astype(F32)
    arrived(att_in, in_r.at[AT])
    for d in range(1, nx):
        total = total + att_in[d - 1].astype(F32)
    res_v[...] = total
    rq = total.astype(BF16)
    tb[0] = rq
    res16[x] = rq
    blocks = tb.at[pl.ds(1, nz - 1)]
    for d in far_z:
        send(TZ, tb.at[0], tb.at[nz - d], in_r.at[TZ], z_peer(d), blocks)
    for d in far_x:
        send(RX, res16.at[x], res16.at[x], in_r.at[RX], x_peer(d), att_in)

    arrived(others, in_r.at[INFO])
    many = nz * rows
    lanes = take.shape[0]
    facts = info[...].reshape(nz * 8, 128)
    facts = jnp.concatenate([facts, jnp.zeros((128 - nz * 8, 128), F32)], axis=0).T
    names = jnp.concatenate([facts[0:rows, d * 8 : d * 8 + 8] for d in range(nz)], axis=0)
    shares = jnp.concatenate([facts[rows : 2 * rows, d * 8 : d * 8 + 8] for d in range(nz)], axis=0)
    lane = lax.broadcasted_iota(jnp.int32, (many, lanes), 1).astype(F32)
    tok_id = lax.broadcasted_iota(jnp.int32, (many, lanes), 0).astype(F32)
    l_group = jnp.floor((lane + 0.5) * (1.0 / part))
    in_group = lane - l_group * part
    l_block = jnp.floor((in_group + 0.5) * (1.0 / CAP))
    l_rank = in_group - l_block * CAP
    l_dy = jnp.floor((l_group + 0.25) * 0.5)
    l_y = y.astype(F32) + l_dy
    l_y = jnp.where(l_y >= ny, l_y - ny, l_y)
    l_c = c.astype(F32) + (l_group - 2.0 * l_dy)
    l_c = jnp.where(l_c >= 2.0, l_c - 2.0, l_c)
    l_expert = (z.astype(F32) * ny + l_y) * 2.0 + l_c
    l_expert = jnp.where(lane < slots, l_expert, -1.0)
    hits = jnp.zeros((many, lanes), F32)
    weigh = jnp.zeros((many, lanes), F32)
    for r in range(top):
        same = names[:, r : r + 1] == l_expert
        hits = jnp.where(same, 1.0, hits)
        weigh = jnp.where(same, shares[:, r : r + 1], weigh)
    t_block = jnp.floor((tok_id + 0.5) * (1.0 / rows))
    row_t = lax.broadcasted_iota(jnp.int32, (many, many), 0).astype(F32)
    col_t = lax.broadcasted_iota(jnp.int32, (many, many), 1).astype(F32)
    before = jnp.where(
        (jnp.floor((row_t + 0.5) * (1.0 / rows)) == jnp.floor((col_t + 0.5) * (1.0 / rows)))
        & (col_t < row_t),
        1.0,
        0.0,
    ).astype(BF16)
    rank = mm(before, hits.astype(BF16))
    chosen = (hits > 0.5) & (rank == l_rank) & (t_block == l_block)
    take[...] = jnp.where(chosen, 1.0, 0.0).T.astype(BF16)
    weigh = jnp.where(chosen, weigh, 0.0)
    high = weigh.astype(BF16)
    comb[0] = high
    comb[1] = (weigh - high.astype(F32)).astype(BF16)

    arrived(columns, in_r.at[SZ])
    three = sgu_v.at[:, :, pl.ds(0, 3), 0]
    near = sgu_v.at[:, :, y, c]
    for d in (1, ny - 1):
        send(SY, near, near, in_r.at[SY], g_peer(2 * d), three)

    arrived(blocks, in_r.at[TZ])
    picked = mm(take[0:slots, :], tb[...].reshape(many, quarter))
    xs[x, 0] = picked[0:part].astype(BF16)
    for g in [2 * d + k for d in far_y for k in range(2)] + [1]:
        slot_out[g - 1] = picked[g * part : (g + 1) * part].astype(BF16)
        send(SL, slot_out.at[g - 1], xs.at[x, g_back(g)], sl_r.at[g_back(g)], g_peer(g), slot_out)
    order = [0, 1] + [2 * d + k for d in reversed(far_y) for k in range(2)]
    right, left = (x + 1) % nx, (x + nx - 1) % nx
    pairs = [order[i : i + 2] for i in range(0, groups, 2)]
    direct = pairs[-1]
    rightward = [s for at, s in enumerate(order) if at in RIGHT]
    chunks = xs.at[pl.ds(0, 3)]

    def rest(s):
        return xc_r.at[order.index(s) // 2]

    def gather_send(s):
        here = xs.at[x, s]
        for d in far_x if s in direct else (1, nx - 1):
            first = s not in direct and (d == 1) == (s in rightward)
            send(XF, here, here, xf_r.at[s] if first else rest(s), x_peer(d), chunks)

    def gather_pass(s):
        here = xs.at[left if s in rightward else right, s]
        arrived(here, xf_r.at[s])
        send(XF, here, here, rest(s), x_peer(1 if s in rightward else nx - 1), chunks)

    parts = ys.at[pl.ds(0, 3)]

    def sum_send(s):
        if s in direct:
            for d in far_x:
                send(YX, ys.at[(x + d) % nx, s], ys_in.at[s, d - 1], yn_r.at[s], x_peer(d), parts)
            return
        on, off = (1, nx - 1) if s in rightward else (nx - 1, 1)
        send(YX, ys.at[(x + 2) % nx, s], opp_in.at[s], yo_r.at[s], x_peer(on), parts)
        send(YX, ys.at[(x + off) % nx, s], ys_in.at[s, 0], yn_r.at[s], x_peer(off), parts)

    def sum_pass(s):
        on = 1 if s in rightward else nx - 1
        arrived(opp_in.at[s], yo_r.at[s])
        opp_out[s] = (ys[(x + on) % nx, s].astype(F32) + opp_in[s].astype(F32)).astype(BF16)
        send(YX, opp_out.at[s], ys_in.at[s, 1], yn_r.at[s], x_peer(on), parts)

    def sum_end(s):
        count = nx - 1 if s in direct else 2
        arrived(ys_in.at[s, pl.ds(0, count)], yn_r.at[s])
        total = ys[x, s].astype(F32)
        for i in range(count):
            total = total + ys_in[s, i].astype(F32)
        if s == 0:
            ret[0] = total.astype(BF16)
        else:
            yy[s - 1] = total.astype(BF16)
            send(YG, yy.at[s - 1], ret.at[g_back(s)], in_r.at[YG], g_peer(s), yy)

    def experts(some):
        arrived(xs.at[0, pl.ds(0, 6 if some == direct else 4)], rest(some[0]))
        pieces = [
            jnp.concatenate([xs[i, s].astype(F32) for s in some], axis=0) for i in range(nx)
        ]
        square = sum(jnp.sum(m * m, axis=-1, keepdims=True) for m in pieces)
        scale = lax.rsqrt(square * (1.0 / width) + EPS)
        feats = jnp.concatenate(
            [(pieces[i] * scale * gain[i]).astype(BF16) for i in range(nx)], axis=1
        )
        hidden = (silu(mm(feats, eg_v[...])) * mm(feats, eu_v[...])).astype(BF16)
        for i in range(nx):
            term = mm(hidden, ed_v[:, i * quarter : (i + 1) * quarter])
            for j, s in enumerate(some):
                ys[i, s] = term[j * part : (j + 1) * part].astype(BF16)
        for s in some:
            sum_send(s)

    local["fgain"].wait()
    local["gv"].wait()
    gain = [fgain_v[:, i * quarter : (i + 1) * quarter] for i in range(nx)]
    for name in ("eg", "eu", "ed"):
        local[name].wait()

    gather_send(0)
    arrived(xs.at[x, 1], sl_r.at[1])
    gather_send(1)
    gather_pass(0)
    for at, s in enumerate(order[2:]):
        arrived(xs.at[x, s], sl_r.at[s])
        gather_send(s)
        if at == 1:
            gather_pass(1)
    for s in pairs[1]:
        gather_pass(s)
    experts(pairs[0])
    arrived(sgu_v.at[:, :, pl.ds(0, 2), 0], in_r.at[SY])
    mid = nz // 2
    low_half = sgu_v.at[:, pl.ds(0, mid), (y + ny - 1) % ny, c]
    high_half = sgu_v.at[:, pl.ds(mid, mid), (y + 1) % ny, c]
    send(SY, low_half, low_half, in_r.at[SC], g_peer(2), three)
    send(SY, high_half, high_half, in_r.at[SC], g_peer(2 * (ny - 1)), three)
    for s in order[4:-2]:
        gather_pass(s)
    experts(pairs[1])
    for s in pairs[0]:
        sum_pass(s)
    for pair in pairs[2:]:
        experts(pair)
    for s in order[2:-2]:
        sum_pass(s)

    arrived(near, in_r.at[SC])
    half = sgu_v.at[:, :, :, c]
    send(SC, half, half, in_r.at[SH], g_peer(1), sgu_v.at[:, :, :, 0])
    for s in order:
        sum_end(s)

    arrived(att_in, in_r.at[RX])
    mine = [res16[i].astype(F32) for i in range(nx)]
    square = sum(jnp.sum(m * m, axis=-1, keepdims=True) for m in mine)
    scale = lax.rsqrt(square * (1.0 / width) + EPS)
    mix = [(mine[i] * scale * gain[i]).astype(BF16) for i in range(nx)]
    joined = jnp.concatenate(mix, axis=1)
    gv = gv_v[...].astype(F32)
    mix_gate = sum(
        joined[:, i * 128 : (i + 1) * 128].astype(F32) * gv[i : i + 1] for i in range(width // 128)
    )
    mix_gate = jnp.sum(mix_gate, axis=-1, keepdims=True)
    mix_gate = 1.0 / (1.0 + jnp.exp(-mix_gate))
    arrived(half, in_r.at[SH])
    local["sd"].wait()
    s_width = sgu_v.shape[-1]
    s_gate = mm(joined, sgu_v[0].reshape(width, s_width))
    s_up = mm(joined, sgu_v[1].reshape(width, s_width))
    s_hidden = (silu(s_gate) * s_up).astype(BF16)
    for i in range(nx):
        sh_out[i] = mm(s_hidden, sd_v[:, i * quarter : (i + 1) * quarter]).astype(BF16)
    for d in far_x:
        send(SH, sh_out.at[(x + d) % nx], sh_in.at[d - 1], in_r.at[ZB], x_peer(d), sh_in)

    arrived(ret.at[pl.ds(1, groups - 1)], in_r.at[YG])
    home = jnp.concatenate([ret[g].astype(F32) for g in range(groups)], axis=0).astype(BF16)
    routed = mm(comb[0][:, 0:slots], home) + mm(comb[1][:, 0:slots], home)
    for d in far_z:
        zs[d - 1] = routed[d * rows : (d + 1) * rows].astype(BF16)
        send(ZB, zs.at[d - 1], zs_in.at[d - 1], in_r.at[LAST], z_peer(d), zs)

    arrived(sh_in, in_r.at[ZB])
    shared = sh_out[x].astype(F32)
    for d in range(1, nx):
        shared = shared + sh_in[d - 1].astype(F32)
    final = res_v[...] + mix_gate * shared + routed[0:rows]
    arrived(zs_in, in_r.at[LAST])
    for d in range(1, nz):
        final = final + zs_in[d - 1].astype(F32)
    layer_out[...] = final.astype(BF16)
    for step, total in posted.items():
        arrived(total, out_s.at[step])


def shards(nz, ny, *args):
    (
        tokens,
        lengths,
        cache,
        attn_gain,
        query_weight,
        key_weight,
        value_weight,
        stick_bias,
        out_weight,
        ffn_gain,
        routes,
        route_weights,
        expert_gate,
        expert_up,
        expert_down,
        shared_gate,
        shared_up,
        shared_down,
        gate_vector,
    ) = args
    nx = lax.axis_size("tp")
    rows, width = tokens.shape
    quarter = width // nx
    groups = 2 * ny
    part = CAP * nz
    slots = groups * part
    lanes = -(-slots // 128) * 128
    heads = query_weight.shape[1] // HEAD_DIM
    length = cache.shape[1]
    vm = pltpu.VMEM
    dma = pltpu.SemaphoreType.DMA

    def like(a):
        return vm(a.shape, a.dtype)

    key_weight, value_weight = key_weight.T, value_weight.T
    routes, route_weights = routes.T, route_weights.T
    attn_gain = attn_gain.reshape(1, width)
    ffn_gain = ffn_gain.reshape(1, width)
    gate_vector = gate_vector.reshape(width // 128, 128)
    scratch = [
        pltpu.SMEM(lengths.shape, lengths.dtype),
        pltpu.SMEM(stick_bias.shape, stick_bias.dtype),
        like(tokens),
        vm((rows, quarter), BF16),
        like(attn_gain),
        like(ffn_gain),
        like(gate_vector),
        like(routes),
        like(route_weights),
        like(query_weight),
        like(key_weight),
        like(value_weight),
        like(out_weight),
        vm(expert_gate.shape[1:], BF16),
        vm(expert_up.shape[1:], BF16),
        vm(expert_down.shape[1:], BF16),
        like(shared_down),
        like(cache),
        vm((2, nz, ny, 2, *shared_gate.shape), BF16),
        vm((rows * heads, 2 * HEAD_DIM), F32),
        vm((rows * heads, 128), jnp.int32),
        vm((rows * heads, length), F32),
        vm((rows * heads, 2 * HEAD_DIM), F32),
        vm((nz, 8, 128), F32),
        vm((lanes, nz * rows), BF16),
        vm((2, nz * rows, lanes), BF16),
        vm((nx, rows, quarter), BF16),
        vm((nx - 1, rows, quarter), BF16),
        vm((rows, quarter), F32),
        vm((nx, rows, quarter), BF16),
        vm((nz, rows, quarter), BF16),
        vm((groups - 1, part, quarter), BF16),
        vm((nx, groups, part, quarter), BF16),
        vm((nx, groups, part, quarter), BF16),
        vm((groups, 3, part, quarter), BF16),
        vm((groups, part, quarter), BF16),
        vm((groups, part, quarter), BF16),
        vm((groups - 1, part, quarter), BF16),
        vm((groups, part, quarter), BF16),
        vm((nz - 1, rows, quarter), BF16),
        vm((nz - 1, rows, quarter), BF16),
        vm((nx, rows, quarter), BF16),
        vm((nx - 1, rows, quarter), BF16),
        dma((24,)),
        dma((4,)),
    ]
    scratch += [dma((13,)), dma((13,))] + [dma((groups,)) for _ in range(5)]
    spaces = [pltpu.HBM] * 19
    operands = (
        tokens,
        lengths,
        cache,
        attn_gain,
        query_weight,
        key_weight,
        value_weight,
        stick_bias,
        out_weight,
        ffn_gain,
        routes,
        route_weights,
        expert_gate,
        expert_up,
        expert_down,
        shared_gate,
        shared_up,
        shared_down,
        gate_vector,
    )
    return pl.pallas_call(
        functools.partial(kernel, (nz, ny, nx)),
        out_shape=(
            jax.ShapeDtypeStruct((rows, quarter), BF16),
            jax.ShapeDtypeStruct((rows, 2 * HEAD_DIM), BF16),
        ),
        in_specs=[pl.BlockSpec(memory_space=s) for s in spaces],
        out_specs=(
            pl.BlockSpec(memory_space=pltpu.VMEM),
            pl.BlockSpec(memory_space=pltpu.VMEM),
        ),
        scratch_shapes=scratch,
        compiler_params=pltpu.CompilerParams(
            collective_id=0, has_side_effects=True, vmem_limit_bytes=48 * 1024 * 1024
        ),
    )(*[pltpu.with_memory_space_constraint(a, pltpu.HBM) for a in operands])


def solution(mesh, ny=NY):
    nz = mesh.shape["ep"] // (2 * ny)
    placed = (
        P("ep", None),
        P("ep"),
        P("ep", None, "tp"),
        P(),
        P(None, "tp"),
        P(None, "tp"),
        P(None, "tp"),
        P("tp"),
        P("tp", None),
        P(),
        P("ep", None),
        P("ep", None),
        P("ep", None, "tp"),
        P("ep", None, "tp"),
        P("ep", "tp", None),
        P("ep", "tp"),
        P("ep", "tp"),
        P("tp", None),
        P(),
    )
    return jax.shard_map(
        functools.partial(shards, nz, ny),
        mesh=mesh,
        in_specs=placed,
        out_specs=(P("ep", "tp"), P("ep", "tp")),
        check_vma=False,
    )
```

```python
import functools

import jax
import jax.numpy as jnp
from jax import lax
from jax.experimental import pallas as pl
from jax.experimental.pallas import tpu as pltpu
from jax.sharding import PartitionSpec as P

HEAD_DIM = 64
EPS = 1e-06
CAP = 3
NY = 4
GATHER_RIGHT = (1, 3, 5, 7)
SUM_RIGHT = (0, 1, 4, 5)
SUM_DIRECT = 1
F32 = jnp.float32
BF16 = jnp.bfloat16
MESH = pl.DeviceIdType.MESH
NT = (((1,), (1,)), ((), ()))


def mm(a, b):
    return jnp.dot(a, b, preferred_element_type=F32)


def mm_nt(a, b):
    return lax.dot_general(a, b, NT, preferred_element_type=F32)


def silu(v):
    return v / (1.0 + jnp.exp(-v))


def kernel(
    dims,
    tokens,
    lengths,
    cache,
    attn_gain,
    query_weight,
    key_weight,
    value_weight,
    stick_bias,
    out_weight,
    ffn_gain,
    routes,
    route_weights,
    expert_gate,
    expert_up,
    expert_down,
    shared_gate,
    shared_up,
    shared_down,
    gate_vector,
    layer_out,
    new_kv,
    len_m,
    bias_m,
    tok_v,
    tokq_v,
    again_v,
    fgain_v,
    gv_v,
    routes_v,
    rw_v,
    wq_v,
    wk_v,
    wv_v,
    wo_v,
    eg_v,
    eu_v,
    ed_v,
    sd_v,
    cache_v,
    sgu_v,
    qrow,
    lrow,
    score,
    orow,
    info,
    take,
    comb,
    att,
    att_in,
    res_v,
    res16,
    tb,
    slot_out,
    xs,
    ys,
    ys_in,
    opp_in,
    opp_out,
    yy,
    ret,
    zs,
    zs_in,
    sh_out,
    sh_in,
    lsem,
    csem,
    out_s,
    in_r,
    sl_r,
    xf_r,
    yo_r,
    yn_r,
    xc_r,
):
    nz, ny, nx = dims
    rows, width = tok_v.shape
    quarter = width // nx
    groups = 2 * ny
    part = CAP * nz
    slots = groups * part
    heads = wq_v.shape[1] // HEAD_DIM
    length = cache_v.shape[1]
    ep = lax.axis_index("ep")
    x = lax.axis_index("tp")
    c = ep % 2
    y = (ep // 2) % ny
    z = ep // (2 * ny)

    def device(z_, y_, c_, x_):
        return ((z_ * ny + y_) * 2 + c_, x_)

    def z_peer(d):
        return device((z + d) % nz, y, c, x)

    def g_peer(g):
        return device(z, (y + g // 2) % ny, (c + g % 2) % 2, x)

    def g_back(g):
        return ((ny - g // 2) % ny) * 2 + g % 2

    def x_peer(d):
        return device(z, y, c, (x + d) % nx)

    def remote(src, dst, send, recv, to):
        copy = pltpu.make_async_remote_copy(
            src_ref=src,
            dst_ref=dst,
            send_sem=send,
            recv_sem=recv,
            device_id=to,
            device_id_type=MESH,
        )
        return copy

    peers = (
        [z_peer(d) for d in range(1, nz)]
        + [g_peer(g) for g in range(1, groups)]
        + [x_peer(d) for d in range(1, nx)]
    )
    local = {}

    def fetch(name, src, dst):
        copy = pltpu.make_async_copy(src, dst, lsem.at[len(local)])
        copy.start()
        local[name] = copy

    own_q = pl.multiple_of(x * quarter, quarter)
    fetch("tok", tokens, tok_v)
    fetch("again", attn_gain, again_v)
    fetch("wq", query_weight, wq_v)
    fetch("wk", key_weight, wk_v)
    fetch("wv", value_weight, wv_v)
    fetch("len", lengths, len_m)
    fetch("bias", stick_bias, bias_m)
    fetch("routes", routes, routes_v)
    fetch("rw", route_weights, rw_v)
    barrier = pltpu.get_barrier_semaphore()
    for peer in peers:
        pl.semaphore_signal(barrier, inc=1, device_id=peer, device_id_type=MESH)

    local["tok"].wait()
    local["again"].wait()
    chunk = rows // 4
    cached = []
    for n in range(4):
        at = pl.ds(n * chunk, chunk)
        copy = pltpu.make_async_copy(cache.at[at], cache_v.at[at], csem.at[n])
        copy.start()
        cached.append(copy)
    tf = tok_v[...].astype(F32)
    normed = (
        tf * lax.rsqrt(jnp.mean(tf * tf, axis=-1, keepdims=True) + EPS) * again_v[...]
    ).astype(BF16)
    local["wq"].wait()
    q = mm(normed, wq_v[...]).astype(BF16).astype(F32)
    local["wk"].wait()
    local["wv"].wait()
    new_kv[...] = jnp.concatenate(
        [mm_nt(normed, wk_v[...]), mm_nt(normed, wv_v[...])], axis=1
    ).astype(BF16)
    for h in range(heads):
        qrow[pl.ds(h, rows, stride=heads), :] = jnp.concatenate(
            [q[:, h * HEAD_DIM : (h + 1) * HEAD_DIM], jnp.zeros((rows, HEAD_DIM), F32)], axis=1
        )
    fetch("wo", out_weight, wo_v)
    fetch("tokq", tokens.at[:, pl.ds(own_q, quarter)], tokq_v)
    fetch("fgain", ffn_gain, fgain_v)
    fetch("gv", gate_vector, gv_v)
    fetch("sg", shared_gate, sgu_v.at[0, z, y, c])
    fetch("su", shared_up, sgu_v.at[1, z, y, c])
    fetch("eg", expert_gate.at[0], eg_v)
    fetch("eu", expert_up.at[0], eu_v)
    fetch("sd", shared_down, sd_v)
    fetch("ed", expert_down.at[0], ed_v)
    local["routes"].wait()
    local["rw"].wait()
    top = routes_v.shape[0]
    info[0] = jnp.concatenate(
        [
            jnp.concatenate(
                [routes_v[...].astype(F32), rw_v[...], jnp.zeros((top, 128 - 2 * rows), F32)], axis=1
            ),
            jnp.zeros((8 - top, 128), F32),
        ],
        axis=0,
    )

    INFO, SZ, SY, SC, AT, RX, TZ, SL, XF, YX, YG, SH, ZB = range(13)
    LAST = SL
    posted = {}

    def send(step, src, dst, recv, to, total):
        posted[step] = total
        remote(src, dst, out_s.at[step], recv, to).start()

    def arrived(ref, sem):
        pltpu.make_async_copy(ref, ref, sem).wait()

    far_z = sorted(range(1, nz), key=lambda d: -min(d, nz - d))
    far_y = sorted(range(1, ny), key=lambda d: -min(d, ny - d))
    far_x = sorted(range(1, nx), key=lambda d: -min(d, nx - d))
    local["len"].wait()
    local["bias"].wait()
    for n in range(rows):
        if n % chunk == 0:
            cached[n // chunk].wait()
        at = slice(n * heads, (n + 1) * heads)
        score[at, :] = mm_nt(qrow[at, :].astype(BF16), cache_v[n])
        lrow[at, :] = jnp.full((heads, 128), len_m[n], jnp.int32)

    block = 256
    table_r = lax.broadcasted_iota(jnp.int32, (block, block), 0)
    table_c = lax.broadcasted_iota(jnp.int32, (block, block), 1)
    later = jnp.where(table_r > table_c, 1.0, 0.0).astype(BF16)
    all_rows = rows * heads
    head_of = lax.broadcasted_iota(jnp.int32, (all_rows, block), 0) & (heads - 1)
    offset = jnp.zeros((all_rows, block), F32)
    for h in range(heads):
        offset = jnp.where(head_of == h, bias_m[h], offset)
    limit = jnp.concatenate([lrow[...]] * (block // 128), axis=1)
    beyond = jnp.zeros((all_rows, 1), F32)
    for b in reversed(range(length // block)):
        at = slice(b * block, (b + 1) * block)
        zv = score[:, at] * HEAD_DIM ** (-0.5) + offset
        soft = jnp.log1p(jnp.exp(-jnp.abs(zv)))
        usable = (lax.broadcasted_iota(jnp.int32, (all_rows, block), 1) + b * block) < limit
        keep = jnp.where(usable, jnp.minimum(-zv, 0.0) - soft, 0.0)
        high = keep.astype(BF16)
        low = (keep - high.astype(F32)).astype(BF16)
        within = mm(high, later) + mm(low, later)
        score[:, at] = jnp.where(
            usable, jnp.exp(jnp.minimum(zv, 0.0) - soft + within + beyond), 0.0
        )
        beyond = beyond + within[:, 0:1] + keep[:, 0:1]

    for n in range(rows):
        at = slice(n * heads, (n + 1) * heads)
        orow[at, :] = mm(score[at, :].astype(BF16), cache_v[n])
    heads_out = jnp.concatenate(
        [orow[pl.ds(h, rows, stride=heads), :][:, HEAD_DIM : 2 * HEAD_DIM] for h in range(heads)],
        axis=1,
    ).astype(BF16)
    local["wo"].wait()
    for i in range(nx):
        at = slice(i * quarter, (i + 1) * quarter)
        att[i] = mm(heads_out, wo_v[:, at]).astype(BF16)

    pl.semaphore_wait(barrier, len(peers))
    for d in far_x:
        send(AT, att.at[(x + d) % nx], att_in.at[d - 1], in_r.at[AT], x_peer(d), att_in)
    others = info.at[pl.ds(1, nz - 1)]
    for d in far_z:
        send(INFO, info.at[0], info.at[nz - d], in_r.at[INFO], z_peer(d), others)

    local["tokq"].wait()
    total = tokq_v[...].astype(F32) + att[x].astype(F32)
    arrived(att_in, in_r.at[AT])
    for d in range(1, nx):
        total = total + att_in[d - 1].astype(F32)
    res_v[...] = total
    rq = total.astype(BF16)
    tb[0] = rq
    res16[x] = rq
    blocks = tb.at[pl.ds(1, nz - 1)]
    for d in far_z:
        send(TZ, tb.at[0], tb.at[nz - d], in_r.at[TZ], z_peer(d), blocks)
    for d in far_x:
        send(RX, res16.at[x], res16.at[x], in_r.at[RX], x_peer(d), att_in)

    arrived(others, in_r.at[INFO])
    many = nz * rows
    lanes = take.shape[0]
    facts = info[...].reshape(nz * 8, 128)
    facts = jnp.concatenate([facts, jnp.zeros((128 - nz * 8, 128), F32)], axis=0).T
    names = jnp.concatenate([facts[0:rows, d * 8 : d * 8 + 8] for d in range(nz)], axis=0)
    shares = jnp.concatenate([facts[rows : 2 * rows, d * 8 : d * 8 + 8] for d in range(nz)], axis=0)
    lane = lax.broadcasted_iota(jnp.int32, (many, lanes), 1).astype(F32)
    tok_id = lax.broadcasted_iota(jnp.int32, (many, lanes), 0).astype(F32)
    l_group = jnp.floor((lane + 0.5) * (1.0 / part))
    in_group = lane - l_group * part
    l_block = jnp.floor((in_group + 0.5) * (1.0 / CAP))
    l_rank = in_group - l_block * CAP
    l_dy = jnp.floor((l_group + 0.25) * 0.5)
    l_y = y.astype(F32) + l_dy
    l_y = jnp.where(l_y >= ny, l_y - ny, l_y)
    l_c = c.astype(F32) + (l_group - 2.0 * l_dy)
    l_c = jnp.where(l_c >= 2.0, l_c - 2.0, l_c)
    l_expert = (z.astype(F32) * ny + l_y) * 2.0 + l_c
    l_expert = jnp.where(lane < slots, l_expert, -1.0)
    hits = jnp.zeros((many, lanes), F32)
    weigh = jnp.zeros((many, lanes), F32)
    for r in range(top):
        same = names[:, r : r + 1] == l_expert
        hits = jnp.where(same, 1.0, hits)
        weigh = jnp.where(same, shares[:, r : r + 1], weigh)
    t_block = jnp.floor((tok_id + 0.5) * (1.0 / rows))
    row_t = lax.broadcasted_iota(jnp.int32, (many, many), 0).astype(F32)
    col_t = lax.broadcasted_iota(jnp.int32, (many, many), 1).astype(F32)
    before = jnp.where(
        (jnp.floor((row_t + 0.5) * (1.0 / rows)) == jnp.floor((col_t + 0.5) * (1.0 / rows)))
        & (col_t < row_t),
        1.0,
        0.0,
    ).astype(BF16)
    rank = mm(before, hits.astype(BF16))
    chosen = (hits > 0.5) & (rank == l_rank) & (t_block == l_block)
    take[...] = jnp.where(chosen, 1.0, 0.0).T.astype(BF16)
    weigh = jnp.where(chosen, weigh, 0.0)
    high = weigh.astype(BF16)
    comb[0] = high
    comb[1] = (weigh - high.astype(F32)).astype(BF16)

    arrived(blocks, in_r.at[TZ])
    picked = mm(take[0:slots, :], tb[...].reshape(many, quarter))
    xs[x, 0] = picked[0:part].astype(BF16)
    for g in [1] + [2 * d + k for d in reversed(far_y) for k in range(2)]:
        slot_out[g - 1] = picked[g * part : (g + 1) * part].astype(BF16)
        send(SL, slot_out.at[g - 1], xs.at[x, g_back(g)], sl_r.at[g_back(g)], g_peer(g), slot_out)
    order = [0, 1] + [2 * d + k for d in reversed(far_y) for k in range(2)]
    right, left = (x + 1) % nx, (x + nx - 1) % nx
    pairs = [order[i : i + 2] for i in range(0, groups, 2)]
    direct = sum(pairs[len(pairs) - SUM_DIRECT :], [])
    gather_right = [s for at, s in enumerate(order) if at in GATHER_RIGHT]
    sum_right = [s for at, s in enumerate(order) if at in SUM_RIGHT]
    chunks = xs.at[pl.ds(0, 3)]

    def rest(s):
        return xc_r.at[order.index(s) // 2]

    def gather_send(s):
        here = xs.at[x, s]
        for d in (1, nx - 1):
            first = (d == 1) == (s in gather_right)
            send(XF, here, here, xf_r.at[s] if first else rest(s), x_peer(d), chunks)

    def gather_pass(s):
        here = xs.at[left if s in gather_right else right, s]
        arrived(here, xf_r.at[s])
        send(XF, here, here, rest(s), x_peer(1 if s in gather_right else nx - 1), chunks)

    parts = ys.at[pl.ds(0, 3)]

    def sum_send(s):
        if s in direct:
            for d in far_x:
                send(YX, ys.at[(x + d) % nx, s], ys_in.at[s, d - 1], yn_r.at[s], x_peer(d), parts)
            return
        on, off = (1, nx - 1) if s in sum_right else (nx - 1, 1)
        send(YX, ys.at[(x + 2) % nx, s], opp_in.at[s], yo_r.at[s], x_peer(on), parts)
        send(YX, ys.at[(x + off) % nx, s], ys_in.at[s, 0], yn_r.at[s], x_peer(off), parts)

    def sum_pass(s):
        on = 1 if s in sum_right else nx - 1
        arrived(opp_in.at[s], yo_r.at[s])
        opp_out[s] = (ys[(x + on) % nx, s].astype(F32) + opp_in[s].astype(F32)).astype(BF16)
        send(YX, opp_out.at[s], ys_in.at[s, 1], yn_r.at[s], x_peer(on), parts)

    def sum_end(s):
        count = nx - 1 if s in direct else 2
        arrived(ys_in.at[s, pl.ds(0, count)], yn_r.at[s])
        total = ys[x, s].astype(F32)
        for i in range(count):
            total = total + ys_in[s, i].astype(F32)
        if s == 0:
            ret[0] = total.astype(BF16)
        else:
            yy[s - 1] = total.astype(BF16)
            send(YG, yy.at[s - 1], ret.at[g_back(s)], in_r.at[YG], g_peer(s), yy)

    def experts(*ready):
        for pair in ready:
            arrived(xs.at[0, pl.ds(0, 4)], rest(pair[0]))
        some = sum(ready, [])
        pieces = [
            jnp.concatenate([xs[i, s].astype(F32) for s in some], axis=0) for i in range(nx)
        ]
        square = sum(jnp.sum(m * m, axis=-1, keepdims=True) for m in pieces)
        scale = lax.rsqrt(square * (1.0 / width) + EPS)
        feats = jnp.concatenate(
            [(pieces[i] * scale * gain[i]).astype(BF16) for i in range(nx)], axis=1
        )
        hidden = (silu(mm(feats, eg_v[...])) * mm(feats, eu_v[...])).astype(BF16)
        for i in range(nx):
            term = mm(hidden, ed_v[:, i * quarter : (i + 1) * quarter])
            for j, s in enumerate(some):
                ys[i, s] = term[j * part : (j + 1) * part].astype(BF16)
        for s in some:
            sum_send(s)

    local["fgain"].wait()
    local["gv"].wait()
    gain = [fgain_v[:, i * quarter : (i + 1) * quarter] for i in range(nx)]
    for name in ("eg", "eu", "ed"):
        local[name].wait()

    local["sg"].wait()
    local["su"].wait()
    columns = sgu_v.at[:, pl.ds(0, nz - 1), 0, 0]
    own = sgu_v.at[:, z, y, c]
    for d in far_z:
        send(SZ, own, own, in_r.at[SZ], z_peer(d), columns)

    gather_send(0)
    arrived(xs.at[x, 1], sl_r.at[1])
    gather_send(1)
    gather_pass(0)
    for at, s in enumerate(order[2:]):
        arrived(xs.at[x, s], sl_r.at[s])
        gather_send(s)
        if at == 1:
            gather_pass(1)
    for s in pairs[1]:
        gather_pass(s)
    experts(pairs[0])
    arrived(columns, in_r.at[SZ])
    three = sgu_v.at[:, :, pl.ds(0, 3), 0]
    near = sgu_v.at[:, :, y, c]
    for d in (1, ny - 1):
        send(SY, near, near, in_r.at[SY], g_peer(2 * d), three)
    for s in order[4:]:
        gather_pass(s)
    experts(pairs[1])
    for s in pairs[0]:
        sum_pass(s)
    experts(*pairs[2:])
    arrived(sgu_v.at[:, :, pl.ds(0, 2), 0], in_r.at[SY])
    mid = nz // 2
    low_half = sgu_v.at[:, pl.ds(0, mid), (y + ny - 1) % ny, c]
    high_half = sgu_v.at[:, pl.ds(mid, mid), (y + 1) % ny, c]
    send(SY, low_half, low_half, in_r.at[SC], g_peer(2), three)
    send(SY, high_half, high_half, in_r.at[SC], g_peer(2 * (ny - 1)), three)
    for s in order[2:]:
        if s not in direct:
            sum_pass(s)

    for s in order[:4] + direct:
        sum_end(s)
    arrived(near, in_r.at[SC])
    half = sgu_v.at[:, :, :, c]
    send(SC, half, half, in_r.at[SH], g_peer(1), sgu_v.at[:, :, :, 0])
    for s in order[4:]:
        if s not in direct:
            sum_end(s)

    arrived(att_in, in_r.at[RX])
    mine = [res16[i].astype(F32) for i in range(nx)]
    square = sum(jnp.sum(m * m, axis=-1, keepdims=True) for m in mine)
    scale = lax.rsqrt(square * (1.0 / width) + EPS)
    mix = [(mine[i] * scale * gain[i]).astype(BF16) for i in range(nx)]
    joined = jnp.concatenate(mix, axis=1)
    gv = gv_v[...].astype(F32)
    mix_gate = sum(
        joined[:, i * 128 : (i + 1) * 128].astype(F32) * gv[i : i + 1] for i in range(width // 128)
    )
    mix_gate = jnp.sum(mix_gate, axis=-1, keepdims=True)
    mix_gate = 1.0 / (1.0 + jnp.exp(-mix_gate))
    arrived(half, in_r.at[SH])
    local["sd"].wait()
    s_width = sgu_v.shape[-1]
    s_gate = mm(joined, sgu_v[0].reshape(width, s_width))
    s_up = mm(joined, sgu_v[1].reshape(width, s_width))
    s_hidden = (silu(s_gate) * s_up).astype(BF16)
    for i in range(nx):
        sh_out[i] = mm(s_hidden, sd_v[:, i * quarter : (i + 1) * quarter]).astype(BF16)
    for d in far_x:
        send(SH, sh_out.at[(x + d) % nx], sh_in.at[d - 1], in_r.at[ZB], x_peer(d), sh_in)

    arrived(ret.at[pl.ds(1, groups - 1)], in_r.at[YG])
    home = jnp.concatenate([ret[g].astype(F32) for g in range(groups)], axis=0).astype(BF16)
    routed = mm(comb[0][:, 0:slots], home) + mm(comb[1][:, 0:slots], home)
    for d in far_z:
        zs[d - 1] = routed[d * rows : (d + 1) * rows].astype(BF16)
        send(ZB, zs.at[d - 1], zs_in.at[d - 1], in_r.at[LAST], z_peer(d), zs)

    arrived(sh_in, in_r.at[ZB])
    shared = sh_out[x].astype(F32)
    for d in range(1, nx):
        shared = shared + sh_in[d - 1].astype(F32)
    final = res_v[...] + mix_gate * shared + routed[0:rows]
    arrived(zs_in, in_r.at[LAST])
    for d in range(1, nz):
        final = final + zs_in[d - 1].astype(F32)
    layer_out[...] = final.astype(BF16)
    for step, total in posted.items():
        arrived(total, out_s.at[step])


def shards(nz, ny, *args):
    (
        tokens,
        lengths,
        cache,
        attn_gain,
        query_weight,
        key_weight,
        value_weight,
        stick_bias,
        out_weight,
        ffn_gain,
        routes,
        route_weights,
        expert_gate,
        expert_up,
        expert_down,
        shared_gate,
        shared_up,
        shared_down,
        gate_vector,
    ) = args
    nx = lax.axis_size("tp")
    rows, width = tokens.shape
    quarter = width // nx
    groups = 2 * ny
    part = CAP * nz
    slots = groups * part
    lanes = -(-slots // 128) * 128
    heads = query_weight.shape[1] // HEAD_DIM
    length = cache.shape[1]
    vm = pltpu.VMEM
    dma = pltpu.SemaphoreType.DMA

    def like(a):
        return vm(a.shape, a.dtype)

    key_weight, value_weight = key_weight.T, value_weight.T
    routes, route_weights = routes.T, route_weights.T
    attn_gain = attn_gain.reshape(1, width)
    ffn_gain = ffn_gain.reshape(1, width)
    gate_vector = gate_vector.reshape(width // 128, 128)
    scratch = [
        pltpu.SMEM(lengths.shape, lengths.dtype),
        pltpu.SMEM(stick_bias.shape, stick_bias.dtype),
        like(tokens),
        vm((rows, quarter), BF16),
        like(attn_gain),
        like(ffn_gain),
        like(gate_vector),
        like(routes),
        like(route_weights),
        like(query_weight),
        like(key_weight),
        like(value_weight),
        like(out_weight),
        vm(expert_gate.shape[1:], BF16),
        vm(expert_up.shape[1:], BF16),
        vm(expert_down.shape[1:], BF16),
        like(shared_down),
        like(cache),
        vm((2, nz, ny, 2, *shared_gate.shape), BF16),
        vm((rows * heads, 2 * HEAD_DIM), F32),
        vm((rows * heads, 128), jnp.int32),
        vm((rows * heads, length), F32),
        vm((rows * heads, 2 * HEAD_DIM), F32),
        vm((nz, 8, 128), F32),
        vm((lanes, nz * rows), BF16),
        vm((2, nz * rows, lanes), BF16),
        vm((nx, rows, quarter), BF16),
        vm((nx - 1, rows, quarter), BF16),
        vm((rows, quarter), F32),
        vm((nx, rows, quarter), BF16),
        vm((nz, rows, quarter), BF16),
        vm((groups - 1, part, quarter), BF16),
        vm((nx, groups, part, quarter), BF16),
        vm((nx, groups, part, quarter), BF16),
        vm((groups, 3, part, quarter), BF16),
        vm((groups, part, quarter), BF16),
        vm((groups, part, quarter), BF16),
        vm((groups - 1, part, quarter), BF16),
        vm((groups, part, quarter), BF16),
        vm((nz - 1, rows, quarter), BF16),
        vm((nz - 1, rows, quarter), BF16),
        vm((nx, rows, quarter), BF16),
        vm((nx - 1, rows, quarter), BF16),
        dma((24,)),
        dma((4,)),
    ]
    scratch += [dma((13,)), dma((13,))] + [dma((groups,)) for _ in range(5)]
    spaces = [pltpu.HBM] * 19
    operands = (
        tokens,
        lengths,
        cache,
        attn_gain,
        query_weight,
        key_weight,
        value_weight,
        stick_bias,
        out_weight,
        ffn_gain,
        routes,
        route_weights,
        expert_gate,
        expert_up,
        expert_down,
        shared_gate,
        shared_up,
        shared_down,
        gate_vector,
    )
    return pl.pallas_call(
        functools.partial(kernel, (nz, ny, nx)),
        out_shape=(
            jax.ShapeDtypeStruct((rows, quarter), BF16),
            jax.ShapeDtypeStruct((rows, 2 * HEAD_DIM), BF16),
        ),
        in_specs=[pl.BlockSpec(memory_space=s) for s in spaces],
        out_specs=(
            pl.BlockSpec(memory_space=pltpu.VMEM),
            pl.BlockSpec(memory_space=pltpu.VMEM),
        ),
        scratch_shapes=scratch,
        compiler_params=pltpu.CompilerParams(
            collective_id=0, has_side_effects=True, vmem_limit_bytes=48 * 1024 * 1024
        ),
    )(*[pltpu.with_memory_space_constraint(a, pltpu.HBM) for a in operands])


def solution(mesh, ny=NY):
    nz = mesh.shape["ep"] // (2 * ny)
    placed = (
        P("ep", None),
        P("ep"),
        P("ep", None, "tp"),
        P(),
        P(None, "tp"),
        P(None, "tp"),
        P(None, "tp"),
        P("tp"),
        P("tp", None),
        P(),
        P("ep", None),
        P("ep", None),
        P("ep", None, "tp"),
        P("ep", None, "tp"),
        P("ep", "tp", None),
        P("ep", "tp"),
        P("ep", "tp"),
        P("tp", None),
        P(),
    )
    return jax.shard_map(
        functools.partial(shards, nz, ny),
        mesh=mesh,
        in_specs=placed,
        out_specs=(P("ep", "tp"), P("ep", "tp")),
        check_vma=False,
    )
```

```python
import functools

import jax
import jax.numpy as jnp
from jax import lax
from jax.experimental import pallas as pl
from jax.experimental.pallas import tpu as pltpu
from jax.sharding import PartitionSpec as P

HEAD_DIM = 64
EPS = 1e-06
CAP = 3
NY = 4
GATHER_RIGHT = (1, 3, 5, 7)
SUM_RIGHT = (0, 1, 4, 5)
SUM_DIRECT = 1
EARLY = 1
F32 = jnp.float32
BF16 = jnp.bfloat16
MESH = pl.DeviceIdType.MESH
NT = (((1,), (1,)), ((), ()))


def mm(a, b):
    return jnp.dot(a, b, preferred_element_type=F32)


def mm_nt(a, b):
    return lax.dot_general(a, b, NT, preferred_element_type=F32)


def silu(v):
    return v / (1.0 + jnp.exp(-v))


def kernel(
    dims,
    tokens,
    lengths,
    cache,
    attn_gain,
    query_weight,
    key_weight,
    value_weight,
    stick_bias,
    out_weight,
    ffn_gain,
    routes,
    route_weights,
    expert_gate,
    expert_up,
    expert_down,
    shared_gate,
    shared_up,
    shared_down,
    gate_vector,
    layer_out,
    new_kv,
    len_m,
    bias_m,
    tok_v,
    tokq_v,
    again_v,
    fgain_v,
    gv_v,
    routes_v,
    rw_v,
    wq_v,
    wk_v,
    wv_v,
    wo_v,
    eg_v,
    eu_v,
    ed_v,
    sd_v,
    cache_v,
    sgu_v,
    qrow,
    lrow,
    score,
    orow,
    info,
    take,
    comb,
    att,
    att_in,
    res_v,
    res16,
    tb,
    slot_out,
    xs,
    ys,
    ys_in,
    opp_in,
    opp_out,
    yy,
    ret,
    zs,
    zs_in,
    sh_out,
    sh_in,
    lsem,
    csem,
    out_s,
    in_r,
    sl_r,
    xf_r,
    yo_r,
    yn_r,
    xc_r,
):
    nz, ny, nx = dims
    rows, width = tok_v.shape
    quarter = width // nx
    groups = 2 * ny
    part = CAP * nz
    slots = groups * part
    heads = wq_v.shape[1] // HEAD_DIM
    length = cache_v.shape[1]
    ep = lax.axis_index("ep")
    x = lax.axis_index("tp")
    c = ep % 2
    y = (ep // 2) % ny
    z = ep // (2 * ny)

    def device(z_, y_, c_, x_):
        return ((z_ * ny + y_) * 2 + c_, x_)

    def z_peer(d):
        return device((z + d) % nz, y, c, x)

    def g_peer(g):
        return device(z, (y + g // 2) % ny, (c + g % 2) % 2, x)

    def g_back(g):
        return ((ny - g // 2) % ny) * 2 + g % 2

    def x_peer(d):
        return device(z, y, c, (x + d) % nx)

    def remote(src, dst, send, recv, to):
        copy = pltpu.make_async_remote_copy(
            src_ref=src,
            dst_ref=dst,
            send_sem=send,
            recv_sem=recv,
            device_id=to,
            device_id_type=MESH,
        )
        return copy

    peers = (
        [z_peer(d) for d in range(1, nz)]
        + [g_peer(g) for g in range(1, groups)]
        + [x_peer(d) for d in range(1, nx)]
    )
    local = {}

    def fetch(name, src, dst):
        copy = pltpu.make_async_copy(src, dst, lsem.at[len(local)])
        copy.start()
        local[name] = copy

    own_q = pl.multiple_of(x * quarter, quarter)
    fetch("tok", tokens, tok_v)
    fetch("again", attn_gain, again_v)
    fetch("len", lengths, len_m)
    fetch("bias", stick_bias, bias_m)
    fetch("routes", routes, routes_v)
    fetch("rw", route_weights, rw_v)
    deep = width // 4
    for i in range(4):
        fetch("wq%d" % i, query_weight.at[pl.ds(i * deep, deep)], wq_v.at[pl.ds(i * deep, deep)])
    chunk = rows // 4

    def fetch_cache(n):
        for m in range(n * chunk, (n + 1) * chunk):
            pltpu.make_async_copy(cache.at[m], cache_v.at[m], csem.at[n]).start()
        at = pl.ds(n * chunk, chunk)
        return pltpu.make_async_copy(cache.at[at], cache_v.at[at], csem.at[n])

    cached = [fetch_cache(n) for n in range(EARLY)]
    barrier = pltpu.get_barrier_semaphore()
    for peer in peers:
        pl.semaphore_signal(barrier, inc=1, device_id=peer, device_id_type=MESH)

    local["tok"].wait()
    local["again"].wait()
    for n in range(EARLY, 4):
        cached.append(fetch_cache(n))
    tf = tok_v[...].astype(F32)
    normed = (
        tf * lax.rsqrt(jnp.mean(tf * tf, axis=-1, keepdims=True) + EPS) * again_v[...]
    ).astype(BF16)
    q = jnp.zeros((rows, wq_v.shape[1]), F32)
    for i in range(4):
        local["wq%d" % i].wait()
        at = slice(i * deep, (i + 1) * deep)
        q = q + mm(normed[:, at], wq_v[at, :])
    q = q.astype(BF16).astype(F32)
    for h in range(heads):
        qrow[pl.ds(h, rows, stride=heads), :] = jnp.concatenate(
            [q[:, h * HEAD_DIM : (h + 1) * HEAD_DIM], jnp.zeros((rows, HEAD_DIM), F32)], axis=1
        )
    fetch("wo", out_weight, wo_v)
    fetch("wk", key_weight, wk_v)
    fetch("wv", value_weight, wv_v)
    fetch("tokq", tokens.at[:, pl.ds(own_q, quarter)], tokq_v)
    fetch("fgain", ffn_gain, fgain_v)
    fetch("gv", gate_vector, gv_v)
    fetch("sg", shared_gate, sgu_v.at[0, z, y, c])
    fetch("su", shared_up, sgu_v.at[1, z, y, c])
    fetch("eg", expert_gate.at[0], eg_v)
    fetch("eu", expert_up.at[0], eu_v)
    fetch("sd", shared_down, sd_v)
    fetch("ed", expert_down.at[0], ed_v)
    INFO, SZ, SY, SC, AT, RX, TZ, SL, XF, YX, YG, SH, ZB = range(13)
    LAST = SL
    posted = {}

    def send(step, src, dst, recv, to, total):
        posted[step] = total
        remote(src, dst, out_s.at[step], recv, to).start()

    def arrived(ref, sem):
        pltpu.make_async_copy(ref, ref, sem).wait()

    far_z = sorted(range(1, nz), key=lambda d: -min(d, nz - d))
    far_y = sorted(range(1, ny), key=lambda d: -min(d, ny - d))
    far_x = sorted(range(1, nx), key=lambda d: -min(d, nx - d))
    local["len"].wait()
    local["bias"].wait()
    for n in range(rows):
        if n % chunk == 0:
            cached[n // chunk].wait()
        at = slice(n * heads, (n + 1) * heads)
        score[at, :] = mm_nt(qrow[at, :].astype(BF16), cache_v[n])
        lrow[at, :] = jnp.full((heads, 128), len_m[n], jnp.int32)

    block = 256
    table_r = lax.broadcasted_iota(jnp.int32, (block, block), 0)
    table_c = lax.broadcasted_iota(jnp.int32, (block, block), 1)
    later = jnp.where(table_r > table_c, 1.0, 0.0).astype(BF16)
    all_rows = rows * heads
    head_of = lax.broadcasted_iota(jnp.int32, (all_rows, block), 0) & (heads - 1)
    offset = jnp.zeros((all_rows, block), F32)
    for h in range(heads):
        offset = jnp.where(head_of == h, bias_m[h], offset)
    limit = jnp.concatenate([lrow[...]] * (block // 128), axis=1)
    beyond = jnp.zeros((all_rows, 1), F32)
    for b in reversed(range(length // block)):
        at = slice(b * block, (b + 1) * block)
        zv = score[:, at] * HEAD_DIM ** (-0.5) + offset
        soft = jnp.log1p(jnp.exp(-jnp.abs(zv)))
        usable = (lax.broadcasted_iota(jnp.int32, (all_rows, block), 1) + b * block) < limit
        keep = jnp.where(usable, jnp.minimum(-zv, 0.0) - soft, 0.0)
        high = keep.astype(BF16)
        low = (keep - high.astype(F32)).astype(BF16)
        within = mm(high, later) + mm(low, later)
        score[:, at] = jnp.where(
            usable, jnp.exp(jnp.minimum(zv, 0.0) - soft + within + beyond), 0.0
        )
        beyond = beyond + within[:, 0:1] + keep[:, 0:1]

    for n in range(rows):
        at = slice(n * heads, (n + 1) * heads)
        orow[at, :] = mm(score[at, :].astype(BF16), cache_v[n])
    heads_out = jnp.concatenate(
        [orow[pl.ds(h, rows, stride=heads), :][:, HEAD_DIM : 2 * HEAD_DIM] for h in range(heads)],
        axis=1,
    ).astype(BF16)
    local["wo"].wait()
    for i in range(nx):
        at = slice(i * quarter, (i + 1) * quarter)
        att[i] = mm(heads_out, wo_v[:, at]).astype(BF16)

    local["routes"].wait()
    local["rw"].wait()
    top = routes_v.shape[0]
    info[0] = jnp.concatenate(
        [
            jnp.concatenate(
                [routes_v[...].astype(F32), rw_v[...], jnp.zeros((top, 128 - 2 * rows), F32)], axis=1
            ),
            jnp.zeros((8 - top, 128), F32),
        ],
        axis=0,
    )
    pl.semaphore_wait(barrier, len(peers))
    for d in far_x:
        send(AT, att.at[(x + d) % nx], att_in.at[d - 1], in_r.at[AT], x_peer(d), att_in)
    others = info.at[pl.ds(1, nz - 1)]
    for d in far_z:
        send(INFO, info.at[0], info.at[nz - d], in_r.at[INFO], z_peer(d), others)

    local["wk"].wait()
    local["wv"].wait()
    new_kv[...] = jnp.concatenate(
        [mm_nt(normed, wk_v[...]), mm_nt(normed, wv_v[...])], axis=1
    ).astype(BF16)
    local["tokq"].wait()
    total = tokq_v[...].astype(F32) + att[x].astype(F32)
    arrived(att_in, in_r.at[AT])
    for d in range(1, nx):
        total = total + att_in[d - 1].astype(F32)
    res_v[...] = total
    rq = total.astype(BF16)
    tb[0] = rq
    res16[x] = rq
    blocks = tb.at[pl.ds(1, nz - 1)]
    for d in far_z:
        send(TZ, tb.at[0], tb.at[nz - d], in_r.at[TZ], z_peer(d), blocks)
    for d in far_x:
        send(RX, res16.at[x], res16.at[x], in_r.at[RX], x_peer(d), att_in)

    arrived(others, in_r.at[INFO])
    many = nz * rows
    lanes = take.shape[0]
    facts = info[...].reshape(nz * 8, 128)
    facts = jnp.concatenate([facts, jnp.zeros((128 - nz * 8, 128), F32)], axis=0).T
    names = jnp.concatenate([facts[0:rows, d * 8 : d * 8 + 8] for d in range(nz)], axis=0)
    shares = jnp.concatenate([facts[rows : 2 * rows, d * 8 : d * 8 + 8] for d in range(nz)], axis=0)
    lane = lax.broadcasted_iota(jnp.int32, (many, lanes), 1).astype(F32)
    tok_id = lax.broadcasted_iota(jnp.int32, (many, lanes), 0).astype(F32)
    l_group = jnp.floor((lane + 0.5) * (1.0 / part))
    in_group = lane - l_group * part
    l_block = jnp.floor((in_group + 0.5) * (1.0 / CAP))
    l_rank = in_group - l_block * CAP
    l_dy = jnp.floor((l_group + 0.25) * 0.5)
    l_y = y.astype(F32) + l_dy
    l_y = jnp.where(l_y >= ny, l_y - ny, l_y)
    l_c = c.astype(F32) + (l_group - 2.0 * l_dy)
    l_c = jnp.where(l_c >= 2.0, l_c - 2.0, l_c)
    l_expert = (z.astype(F32) * ny + l_y) * 2.0 + l_c
    l_expert = jnp.where(lane < slots, l_expert, -1.0)
    hits = jnp.zeros((many, lanes), F32)
    weigh = jnp.zeros((many, lanes), F32)
    for r in range(top):
        same = names[:, r : r + 1] == l_expert
        hits = jnp.where(same, 1.0, hits)
        weigh = jnp.where(same, shares[:, r : r + 1], weigh)
    t_block = jnp.floor((tok_id + 0.5) * (1.0 / rows))
    row_t = lax.broadcasted_iota(jnp.int32, (many, many), 0).astype(F32)
    col_t = lax.broadcasted_iota(jnp.int32, (many, many), 1).astype(F32)
    before = jnp.where(
        (jnp.floor((row_t + 0.5) * (1.0 / rows)) == jnp.floor((col_t + 0.5) * (1.0 / rows)))
        & (col_t < row_t),
        1.0,
        0.0,
    ).astype(BF16)
    rank = mm(before, hits.astype(BF16))
    chosen = (hits > 0.5) & (rank == l_rank) & (t_block == l_block)
    take[...] = jnp.where(chosen, 1.0, 0.0).T.astype(BF16)
    weigh = jnp.where(chosen, weigh, 0.0)
    high = weigh.astype(BF16)
    comb[0] = high
    comb[1] = (weigh - high.astype(F32)).astype(BF16)

    arrived(blocks, in_r.at[TZ])
    picked = mm(take[0:slots, :], tb[...].reshape(many, quarter))
    xs[x, 0] = picked[0:part].astype(BF16)
    for g in [1] + [2 * d + k for d in reversed(far_y) for k in range(2)]:
        slot_out[g - 1] = picked[g * part : (g + 1) * part].astype(BF16)
        send(SL, slot_out.at[g - 1], xs.at[x, g_back(g)], sl_r.at[g_back(g)], g_peer(g), slot_out)
    order = [0, 1] + [2 * d + k for d in reversed(far_y) for k in range(2)]
    right, left = (x + 1) % nx, (x + nx - 1) % nx
    pairs = [order[i : i + 2] for i in range(0, groups, 2)]
    direct = sum(pairs[len(pairs) - SUM_DIRECT :], [])
    gather_right = [s for at, s in enumerate(order) if at in GATHER_RIGHT]
    sum_right = [s for at, s in enumerate(order) if at in SUM_RIGHT]
    chunks = xs.at[pl.ds(0, 3)]

    def rest(s):
        return xc_r.at[order.index(s) // 2]

    def last(s):
        return xc_r.at[(groups + order.index(s)) // 2]

    def gather_send(s):
        here = xs.at[x, s]
        for d in (1, nx - 1):
            first = (d == 1) == (s in gather_right)
            send(XF, here, here, xf_r.at[s] if first else rest(s), x_peer(d), chunks)

    def gather_pass(s):
        here = xs.at[left if s in gather_right else right, s]
        arrived(here, xf_r.at[s])
        send(XF, here, here, last(s), x_peer(1 if s in gather_right else nx - 1), chunks)

    parts = ys.at[pl.ds(0, 3)]

    def sum_send(s):
        if s in direct:
            for d in far_x:
                send(YX, ys.at[(x + d) % nx, s], ys_in.at[s, d - 1], yn_r.at[s], x_peer(d), parts)
            return
        on, off = (1, nx - 1) if s in sum_right else (nx - 1, 1)
        send(YX, ys.at[(x + 2) % nx, s], opp_in.at[s], yo_r.at[s], x_peer(on), parts)
        send(YX, ys.at[(x + off) % nx, s], ys_in.at[s, 0], yn_r.at[s], x_peer(off), parts)

    def sum_pass(s):
        on = 1 if s in sum_right else nx - 1
        arrived(opp_in.at[s], yo_r.at[s])
        opp_out[s] = (ys[(x + on) % nx, s].astype(F32) + opp_in[s].astype(F32)).astype(BF16)
        send(YX, opp_out.at[s], ys_in.at[s, 1], yn_r.at[s], x_peer(on), parts)

    def sum_end(s):
        count = nx - 1 if s in direct else 2
        arrived(ys_in.at[s, pl.ds(0, count)], yn_r.at[s])
        total = ys[x, s].astype(F32)
        for i in range(count):
            total = total + ys_in[s, i].astype(F32)
        if s == 0:
            ret[0] = total.astype(BF16)
        else:
            yy[s - 1] = total.astype(BF16)
            send(YG, yy.at[s - 1], ret.at[g_back(s)], in_r.at[YG], g_peer(s), yy)

    def experts(*ready):
        some = sum(ready, [])
        square = gated = raised = 0.0
        for d in (0, 1, nx - 1, 2):
            if d in (1, 2):
                for pair in ready:
                    arrived(xs.at[0, pl.ds(0, 2)], last(pair[0]) if d == 2 else rest(pair[0]))
            q = (x + d) % nx
            at = pl.ds(pl.multiple_of(q * quarter, quarter), quarter)
            piece = jnp.concatenate([xs[q, s].astype(F32) for s in some], axis=0)
            square = square + jnp.sum(piece * piece, axis=-1, keepdims=True)
            feats = (piece * fgain_v[:, at]).astype(BF16)
            gated = gated + mm(feats, eg_v[at, :])
            raised = raised + mm(feats, eu_v[at, :])
        scale = lax.rsqrt(square * (1.0 / width) + EPS)
        hidden = (silu(gated * scale) * (raised * scale)).astype(BF16)
        for i in range(nx):
            term = mm(hidden, ed_v[:, i * quarter : (i + 1) * quarter])
            for j, s in enumerate(some):
                ys[i, s] = term[j * part : (j + 1) * part].astype(BF16)
        for s in some:
            sum_send(s)

    local["fgain"].wait()
    local["gv"].wait()
    gain = [fgain_v[:, i * quarter : (i + 1) * quarter] for i in range(nx)]
    for name in ("eg", "eu", "ed"):
        local[name].wait()

    local["sg"].wait()
    local["su"].wait()
    columns = sgu_v.at[:, pl.ds(0, nz - 1), 0, 0]
    own = sgu_v.at[:, z, y, c]
    for d in far_z:
        send(SZ, own, own, in_r.at[SZ], z_peer(d), columns)

    gather_send(0)
    arrived(xs.at[x, 1], sl_r.at[1])
    gather_send(1)
    gather_pass(0)
    for at, s in enumerate(order[2:]):
        arrived(xs.at[x, s], sl_r.at[s])
        gather_send(s)
        if at == 1:
            gather_pass(1)
    for s in pairs[1]:
        gather_pass(s)
    experts(pairs[0])
    arrived(columns, in_r.at[SZ])
    three = sgu_v.at[:, :, pl.ds(0, 3), 0]
    near = sgu_v.at[:, :, y, c]
    for d in (1, ny - 1):
        send(SY, near, near, in_r.at[SY], g_peer(2 * d), three)
    for s in order[4:]:
        gather_pass(s)
    experts(pairs[1])
    for s in pairs[0]:
        sum_pass(s)
    experts(*pairs[2:])
    arrived(sgu_v.at[:, :, pl.ds(0, 2), 0], in_r.at[SY])
    mid = nz // 2
    low_half = sgu_v.at[:, pl.ds(0, mid), (y + ny - 1) % ny, c]
    high_half = sgu_v.at[:, pl.ds(mid, mid), (y + 1) % ny, c]
    send(SY, low_half, low_half, in_r.at[SC], g_peer(2), three)
    send(SY, high_half, high_half, in_r.at[SC], g_peer(2 * (ny - 1)), three)
    for s in order[2:]:
        if s not in direct:
            sum_pass(s)

    for s in order[:4] + direct:
        sum_end(s)
    arrived(near, in_r.at[SC])
    half = sgu_v.at[:, :, :, c]
    send(SC, half, half, in_r.at[SH], g_peer(1), sgu_v.at[:, :, :, 0])
    for s in order[4:]:
        if s not in direct:
            sum_end(s)

    arrived(att_in, in_r.at[RX])
    mine = [res16[i].astype(F32) for i in range(nx)]
    square = sum(jnp.sum(m * m, axis=-1, keepdims=True) for m in mine)
    scale = lax.rsqrt(square * (1.0 / width) + EPS)
    mix = [(mine[i] * scale * gain[i]).astype(BF16) for i in range(nx)]
    joined = jnp.concatenate(mix, axis=1)
    gv = gv_v[...].astype(F32)
    mix_gate = sum(
        joined[:, i * 128 : (i + 1) * 128].astype(F32) * gv[i : i + 1] for i in range(width // 128)
    )
    mix_gate = jnp.sum(mix_gate, axis=-1, keepdims=True)
    mix_gate = 1.0 / (1.0 + jnp.exp(-mix_gate))
    arrived(half, in_r.at[SH])
    local["sd"].wait()
    s_width = sgu_v.shape[-1]
    s_gate = mm(joined, sgu_v[0].reshape(width, s_width))
    s_up = mm(joined, sgu_v[1].reshape(width, s_width))
    s_hidden = (silu(s_gate) * s_up).astype(BF16)
    for i in range(nx):
        sh_out[i] = mm(s_hidden, sd_v[:, i * quarter : (i + 1) * quarter]).astype(BF16)
    for d in far_x:
        send(SH, sh_out.at[(x + d) % nx], sh_in.at[d - 1], in_r.at[ZB], x_peer(d), sh_in)

    arrived(ret.at[pl.ds(1, groups - 1)], in_r.at[YG])
    home = jnp.concatenate([ret[g].astype(F32) for g in range(groups)], axis=0).astype(BF16)
    routed = mm(comb[0][:, 0:slots], home) + mm(comb[1][:, 0:slots], home)
    for d in far_z:
        zs[d - 1] = routed[d * rows : (d + 1) * rows].astype(BF16)
        send(ZB, zs.at[d - 1], zs_in.at[d - 1], in_r.at[LAST], z_peer(d), zs)

    arrived(sh_in, in_r.at[ZB])
    shared = sh_out[x].astype(F32)
    for d in range(1, nx):
        shared = shared + sh_in[d - 1].astype(F32)
    final = res_v[...] + mix_gate * shared + routed[0:rows]
    arrived(zs_in, in_r.at[LAST])
    for d in range(1, nz):
        final = final + zs_in[d - 1].astype(F32)
    layer_out[...] = final.astype(BF16)
    for step, total in posted.items():
        arrived(total, out_s.at[step])


def shards(nz, ny, *args):
    (
        tokens,
        lengths,
        cache,
        attn_gain,
        query_weight,
        key_weight,
        value_weight,
        stick_bias,
        out_weight,
        ffn_gain,
        routes,
        route_weights,
        expert_gate,
        expert_up,
        expert_down,
        shared_gate,
        shared_up,
        shared_down,
        gate_vector,
    ) = args
    nx = lax.axis_size("tp")
    rows, width = tokens.shape
    quarter = width // nx
    groups = 2 * ny
    part = CAP * nz
    slots = groups * part
    lanes = -(-slots // 128) * 128
    heads = query_weight.shape[1] // HEAD_DIM
    length = cache.shape[1]
    vm = pltpu.VMEM
    dma = pltpu.SemaphoreType.DMA

    def like(a):
        return vm(a.shape, a.dtype)

    key_weight, value_weight = key_weight.T, value_weight.T
    routes, route_weights = routes.T, route_weights.T
    attn_gain = attn_gain.reshape(1, width)
    ffn_gain = ffn_gain.reshape(1, width)
    gate_vector = gate_vector.reshape(width // 128, 128)
    scratch = [
        pltpu.SMEM(lengths.shape, lengths.dtype),
        pltpu.SMEM(stick_bias.shape, stick_bias.dtype),
        like(tokens),
        vm((rows, quarter), BF16),
        like(attn_gain),
        like(ffn_gain),
        like(gate_vector),
        like(routes),
        like(route_weights),
        like(query_weight),
        like(key_weight),
        like(value_weight),
        like(out_weight),
        vm(expert_gate.shape[1:], BF16),
        vm(expert_up.shape[1:], BF16),
        vm(expert_down.shape[1:], BF16),
        like(shared_down),
        like(cache),
        vm((2, nz, ny, 2, *shared_gate.shape), BF16),
        vm((rows * heads, 2 * HEAD_DIM), F32),
        vm((rows * heads, 128), jnp.int32),
        vm((rows * heads, length), F32),
        vm((rows * heads, 2 * HEAD_DIM), F32),
        vm((nz, 8, 128), F32),
        vm((lanes, nz * rows), BF16),
        vm((2, nz * rows, lanes), BF16),
        vm((nx, rows, quarter), BF16),
        vm((nx - 1, rows, quarter), BF16),
        vm((rows, quarter), F32),
        vm((nx, rows, quarter), BF16),
        vm((nz, rows, quarter), BF16),
        vm((groups - 1, part, quarter), BF16),
        vm((nx, groups, part, quarter), BF16),
        vm((nx, groups, part, quarter), BF16),
        vm((groups, 3, part, quarter), BF16),
        vm((groups, part, quarter), BF16),
        vm((groups, part, quarter), BF16),
        vm((groups - 1, part, quarter), BF16),
        vm((groups, part, quarter), BF16),
        vm((nz - 1, rows, quarter), BF16),
        vm((nz - 1, rows, quarter), BF16),
        vm((nx, rows, quarter), BF16),
        vm((nx - 1, rows, quarter), BF16),
        dma((22,)),
        dma((4,)),
    ]
    scratch += [dma((13,)), dma((13,))] + [dma((groups,)) for _ in range(5)]
    spaces = [pltpu.HBM] * 19
    operands = (
        tokens,
        lengths,
        cache,
        attn_gain,
        query_weight,
        key_weight,
        value_weight,
        stick_bias,
        out_weight,
        ffn_gain,
        routes,
        route_weights,
        expert_gate,
        expert_up,
        expert_down,
        shared_gate,
        shared_up,
        shared_down,
        gate_vector,
    )
    return pl.pallas_call(
        functools.partial(kernel, (nz, ny, nx)),
        out_shape=(
            jax.ShapeDtypeStruct((rows, quarter), BF16),
            jax.ShapeDtypeStruct((rows, 2 * HEAD_DIM), BF16),
        ),
        in_specs=[pl.BlockSpec(memory_space=s) for s in spaces],
        out_specs=(
            pl.BlockSpec(memory_space=pltpu.VMEM),
            pl.BlockSpec(memory_space=pltpu.VMEM),
        ),
        scratch_shapes=scratch,
        compiler_params=pltpu.CompilerParams(
            collective_id=0, has_side_effects=True, vmem_limit_bytes=48 * 1024 * 1024
        ),
    )(*[pltpu.with_memory_space_constraint(a, pltpu.HBM) for a in operands])


def solution(mesh, ny=NY):
    nz = mesh.shape["ep"] // (2 * ny)
    placed = (
        P("ep", None),
        P("ep"),
        P("ep", None, "tp"),
        P(),
        P(None, "tp"),
        P(None, "tp"),
        P(None, "tp"),
        P("tp"),
        P("tp", None),
        P(),
        P("ep", None),
        P("ep", None),
        P("ep", None, "tp"),
        P("ep", None, "tp"),
        P("ep", "tp", None),
        P("ep", "tp"),
        P("ep", "tp"),
        P("tp", None),
        P(),
    )
    return jax.shard_map(
        functools.partial(shards, nz, ny),
        mesh=mesh,
        in_specs=placed,
        out_specs=(P("ep", "tp"), P("ep", "tp")),
        check_vma=False,
    )
```

```python
import functools

import jax
import jax.numpy as jnp
from jax import lax
from jax.experimental import pallas as pl
from jax.experimental.pallas import tpu as pltpu
from jax.sharding import PartitionSpec as P

HEAD_DIM = 64
EPS = 1e-06
CAP = 3
NY = 4
GATHER_RIGHT = (1, 3, 5, 7)
SUM_RIGHT = (0, 1)
SUM_DIRECT = 2
EARLY = 1
F32 = jnp.float32
BF16 = jnp.bfloat16
MESH = pl.DeviceIdType.MESH
NT = (((1,), (1,)), ((), ()))


def mm(a, b):
    return jnp.dot(a, b, preferred_element_type=F32)


def mm_nt(a, b):
    return lax.dot_general(a, b, NT, preferred_element_type=F32)


def silu(v):
    return v / (1.0 + jnp.exp(-v))


def kernel(
    dims,
    tokens,
    lengths,
    cache,
    attn_gain,
    query_weight,
    key_weight,
    value_weight,
    stick_bias,
    out_weight,
    ffn_gain,
    routes,
    route_weights,
    expert_gate,
    expert_up,
    expert_down,
    shared_gate,
    shared_up,
    shared_down,
    gate_vector,
    layer_out,
    new_kv,
    len_m,
    bias_m,
    tok_v,
    tokq_v,
    again_v,
    fgain_v,
    gv_v,
    routes_v,
    rw_v,
    wq_v,
    wk_v,
    wv_v,
    wo_v,
    eg_v,
    eu_v,
    ed_v,
    sd_v,
    cache_v,
    sgu_v,
    qrow,
    lrow,
    score,
    orow,
    info,
    take,
    comb,
    att,
    att_in,
    res_v,
    res16,
    tb,
    slot_out,
    xs,
    ys,
    ys_in,
    opp_in,
    opp_out,
    yy,
    ret,
    zs,
    zs_in,
    sh_out,
    sh_in,
    lsem,
    csem,
    out_s,
    in_r,
    sl_r,
    xf_r,
    yo_r,
    yn_r,
    xc_r,
):
    nz, ny, nx = dims
    rows, width = tok_v.shape
    quarter = width // nx
    groups = 2 * ny
    part = CAP * nz
    slots = groups * part
    heads = wq_v.shape[1] // HEAD_DIM
    length = cache_v.shape[1]
    ep = lax.axis_index("ep")
    x = lax.axis_index("tp")
    c = ep % 2
    y = (ep // 2) % ny
    z = ep // (2 * ny)

    def device(z_, y_, c_, x_):
        return ((z_ * ny + y_) * 2 + c_, x_)

    def z_peer(d):
        return device((z + d) % nz, y, c, x)

    def g_peer(g):
        return device(z, (y + g // 2) % ny, (c + g % 2) % 2, x)

    def g_back(g):
        return ((ny - g // 2) % ny) * 2 + g % 2

    def x_peer(d):
        return device(z, y, c, (x + d) % nx)

    def remote(src, dst, send, recv, to):
        copy = pltpu.make_async_remote_copy(
            src_ref=src,
            dst_ref=dst,
            send_sem=send,
            recv_sem=recv,
            device_id=to,
            device_id_type=MESH,
        )
        return copy

    peers = (
        [z_peer(d) for d in range(1, nz)]
        + [g_peer(g) for g in range(1, groups)]
        + [x_peer(d) for d in range(1, nx)]
    )
    local = {}

    def fetch(name, src, dst):
        copy = pltpu.make_async_copy(src, dst, lsem.at[len(local)])
        copy.start()
        local[name] = copy

    own_q = pl.multiple_of(x * quarter, quarter)
    fetch("tok", tokens, tok_v)
    fetch("again", attn_gain, again_v)
    fetch("len", lengths, len_m)
    fetch("bias", stick_bias, bias_m)
    fetch("routes", routes, routes_v)
    fetch("rw", route_weights, rw_v)
    deep = width // 4
    for i in range(4):
        fetch("wq%d" % i, query_weight.at[pl.ds(i * deep, deep)], wq_v.at[pl.ds(i * deep, deep)])
    chunk = rows // 4

    def fetch_cache(n):
        for m in range(n * chunk, (n + 1) * chunk):
            pltpu.make_async_copy(cache.at[m], cache_v.at[m], csem.at[n]).start()
        at = pl.ds(n * chunk, chunk)
        return pltpu.make_async_copy(cache.at[at], cache_v.at[at], csem.at[n])

    cached = [fetch_cache(n) for n in range(EARLY)]
    barrier = pltpu.get_barrier_semaphore()
    for peer in peers:
        pl.semaphore_signal(barrier, inc=1, device_id=peer, device_id_type=MESH)

    local["tok"].wait()
    local["again"].wait()
    for n in range(EARLY, 4):
        cached.append(fetch_cache(n))
    tf = tok_v[...].astype(F32)
    normed = (
        tf * lax.rsqrt(jnp.mean(tf * tf, axis=-1, keepdims=True) + EPS) * again_v[...]
    ).astype(BF16)
    q = jnp.zeros((rows, wq_v.shape[1]), F32)
    for i in range(4):
        local["wq%d" % i].wait()
        at = slice(i * deep, (i + 1) * deep)
        q = q + mm(normed[:, at], wq_v[at, :])
    q = q.astype(BF16).astype(F32)
    for h in range(heads):
        qrow[pl.ds(h, rows, stride=heads), :] = jnp.concatenate(
            [q[:, h * HEAD_DIM : (h + 1) * HEAD_DIM], jnp.zeros((rows, HEAD_DIM), F32)], axis=1
        )
    fetch("wo", out_weight, wo_v)
    fetch("wk", key_weight, wk_v)
    fetch("wv", value_weight, wv_v)
    fetch("tokq", tokens.at[:, pl.ds(own_q, quarter)], tokq_v)
    fetch("fgain", ffn_gain, fgain_v)
    fetch("gv", gate_vector, gv_v)
    fetch("sg", shared_gate, sgu_v.at[0, z, y, c])
    fetch("su", shared_up, sgu_v.at[1, z, y, c])
    fetch("eg", expert_gate.at[0], eg_v)
    fetch("eu", expert_up.at[0], eu_v)
    fetch("sd", shared_down, sd_v)
    fetch("ed", expert_down.at[0], ed_v)
    INFO, SZ, SY, SC, AT, RX, TZ, SL, XF, YX, YG, SH, ZB = range(13)
    LAST = SL
    posted = {}

    def send(step, src, dst, recv, to, total):
        posted[step] = total
        remote(src, dst, out_s.at[step], recv, to).start()

    def arrived(ref, sem):
        pltpu.make_async_copy(ref, ref, sem).wait()

    far_z = sorted(range(1, nz), key=lambda d: -min(d, nz - d))
    far_y = sorted(range(1, ny), key=lambda d: -min(d, ny - d))
    far_x = sorted(range(1, nx), key=lambda d: -min(d, nx - d))
    local["len"].wait()
    local["bias"].wait()
    for n in range(rows):
        if n % chunk == 0:
            cached[n // chunk].wait()
        at = slice(n * heads, (n + 1) * heads)
        score[at, :] = mm_nt(qrow[at, :].astype(BF16), cache_v[n])
        lrow[at, :] = jnp.full((heads, 128), len_m[n], jnp.int32)

    block = 256
    table_r = lax.broadcasted_iota(jnp.int32, (block, block), 0)
    table_c = lax.broadcasted_iota(jnp.int32, (block, block), 1)
    later = jnp.where(table_r > table_c, 1.0, 0.0).astype(BF16)
    all_rows = rows * heads
    head_of = lax.broadcasted_iota(jnp.int32, (all_rows, block), 0) & (heads - 1)
    offset = jnp.zeros((all_rows, block), F32)
    for h in range(heads):
        offset = jnp.where(head_of == h, bias_m[h], offset)
    limit = jnp.concatenate([lrow[...]] * (block // 128), axis=1)
    beyond = jnp.zeros((all_rows, 1), F32)
    for b in reversed(range(length // block)):
        at = slice(b * block, (b + 1) * block)
        zv = score[:, at] * HEAD_DIM ** (-0.5) + offset
        soft = jnp.log1p(jnp.exp(-jnp.abs(zv)))
        usable = (lax.broadcasted_iota(jnp.int32, (all_rows, block), 1) + b * block) < limit
        keep = jnp.where(usable, jnp.minimum(-zv, 0.0) - soft, 0.0)
        high = keep.astype(BF16)
        low = (keep - high.astype(F32)).astype(BF16)
        within = mm(high, later) + mm(low, later)
        score[:, at] = jnp.where(
            usable, jnp.exp(jnp.minimum(zv, 0.0) - soft + within + beyond), 0.0
        )
        beyond = beyond + within[:, 0:1] + keep[:, 0:1]

    for n in range(rows):
        at = slice(n * heads, (n + 1) * heads)
        orow[at, :] = mm(score[at, :].astype(BF16), cache_v[n])
    heads_out = jnp.concatenate(
        [orow[pl.ds(h, rows, stride=heads), :][:, HEAD_DIM : 2 * HEAD_DIM] for h in range(heads)],
        axis=1,
    ).astype(BF16)
    local["wo"].wait()
    for i in range(nx):
        at = slice(i * quarter, (i + 1) * quarter)
        att[i] = mm(heads_out, wo_v[:, at]).astype(BF16)

    local["routes"].wait()
    local["rw"].wait()
    top = routes_v.shape[0]
    info[0] = jnp.concatenate(
        [
            jnp.concatenate(
                [routes_v[...].astype(F32), rw_v[...], jnp.zeros((top, 128 - 2 * rows), F32)], axis=1
            ),
            jnp.zeros((8 - top, 128), F32),
        ],
        axis=0,
    )
    pl.semaphore_wait(barrier, len(peers))
    for d in far_x:
        send(AT, att.at[(x + d) % nx], att_in.at[d - 1], in_r.at[AT], x_peer(d), att_in)
    others = info.at[pl.ds(1, nz - 1)]
    for d in far_z:
        send(INFO, info.at[0], info.at[nz - d], in_r.at[INFO], z_peer(d), others)

    local["wk"].wait()
    local["wv"].wait()
    new_kv[...] = jnp.concatenate(
        [mm_nt(normed, wk_v[...]), mm_nt(normed, wv_v[...])], axis=1
    ).astype(BF16)
    local["tokq"].wait()
    total = tokq_v[...].astype(F32) + att[x].astype(F32)
    arrived(att_in, in_r.at[AT])
    for d in range(1, nx):
        total = total + att_in[d - 1].astype(F32)
    res_v[...] = total
    rq = total.astype(BF16)
    tb[0] = rq
    res16[x] = rq
    blocks = tb.at[pl.ds(1, nz - 1)]
    for d in far_z:
        send(TZ, tb.at[0], tb.at[nz - d], in_r.at[TZ], z_peer(d), blocks)
    for d in far_x:
        send(RX, res16.at[x], res16.at[x], in_r.at[RX], x_peer(d), att_in)

    arrived(others, in_r.at[INFO])
    many = nz * rows
    lanes = take.shape[0]
    facts = info[...].reshape(nz * 8, 128)
    facts = jnp.concatenate([facts, jnp.zeros((128 - nz * 8, 128), F32)], axis=0).T
    names = jnp.concatenate([facts[0:rows, d * 8 : d * 8 + 8] for d in range(nz)], axis=0)
    shares = jnp.concatenate([facts[rows : 2 * rows, d * 8 : d * 8 + 8] for d in range(nz)], axis=0)
    lane = lax.broadcasted_iota(jnp.int32, (many, lanes), 1).astype(F32)
    tok_id = lax.broadcasted_iota(jnp.int32, (many, lanes), 0).astype(F32)
    l_group = jnp.floor((lane + 0.5) * (1.0 / part))
    in_group = lane - l_group * part
    l_block = jnp.floor((in_group + 0.5) * (1.0 / CAP))
    l_rank = in_group - l_block * CAP
    l_dy = jnp.floor((l_group + 0.25) * 0.5)
    l_y = y.astype(F32) + l_dy
    l_y = jnp.where(l_y >= ny, l_y - ny, l_y)
    l_c = c.astype(F32) + (l_group - 2.0 * l_dy)
    l_c = jnp.where(l_c >= 2.0, l_c - 2.0, l_c)
    l_expert = (z.astype(F32) * ny + l_y) * 2.0 + l_c
    l_expert = jnp.where(lane < slots, l_expert, -1.0)
    hits = jnp.zeros((many, lanes), F32)
    weigh = jnp.zeros((many, lanes), F32)
    for r in range(top):
        same = names[:, r : r + 1] == l_expert
        hits = jnp.where(same, 1.0, hits)
        weigh = jnp.where(same, shares[:, r : r + 1], weigh)
    t_block = jnp.floor((tok_id + 0.5) * (1.0 / rows))
    row_t = lax.broadcasted_iota(jnp.int32, (many, many), 0).astype(F32)
    col_t = lax.broadcasted_iota(jnp.int32, (many, many), 1).astype(F32)
    before = jnp.where(
        (jnp.floor((row_t + 0.5) * (1.0 / rows)) == jnp.floor((col_t + 0.5) * (1.0 / rows)))
        & (col_t < row_t),
        1.0,
        0.0,
    ).astype(BF16)
    rank = mm(before, hits.astype(BF16))
    chosen = (hits > 0.5) & (rank == l_rank) & (t_block == l_block)
    take[...] = jnp.where(chosen, 1.0, 0.0).T.astype(BF16)
    weigh = jnp.where(chosen, weigh, 0.0)
    high = weigh.astype(BF16)
    comb[0] = high
    comb[1] = (weigh - high.astype(F32)).astype(BF16)

    arrived(blocks, in_r.at[TZ])
    picked = mm(take[0:slots, :], tb[...].reshape(many, quarter))
    xs[x, 0] = picked[0:part].astype(BF16)
    for g in [1] + [2 * d + k for d in reversed(far_y) for k in range(2)]:
        slot_out[g - 1] = picked[g * part : (g + 1) * part].astype(BF16)
        send(SL, slot_out.at[g - 1], xs.at[x, g_back(g)], sl_r.at[g_back(g)], g_peer(g), slot_out)
    order = [0, 1] + [2 * d + k for d in reversed(far_y) for k in range(2)]
    right, left = (x + 1) % nx, (x + nx - 1) % nx
    pairs = [order[i : i + 2] for i in range(0, groups, 2)]
    direct = sum(pairs[len(pairs) - SUM_DIRECT :], [])
    gather_right = [s for at, s in enumerate(order) if at in GATHER_RIGHT]
    sum_right = [s for at, s in enumerate(order) if at in SUM_RIGHT]
    chunks = xs.at[pl.ds(0, 3)]

    def rest(s):
        return xc_r.at[order.index(s) // 2]

    def last(s):
        return xc_r.at[(groups + order.index(s)) // 2]

    def gather_send(s):
        here = xs.at[x, s]
        for d in (1, nx - 1):
            first = (d == 1) == (s in gather_right)
            send(XF, here, here, xf_r.at[s] if first else rest(s), x_peer(d), chunks)

    def gather_pass(s):
        here = xs.at[left if s in gather_right else right, s]
        arrived(here, xf_r.at[s])
        send(XF, here, here, last(s), x_peer(1 if s in gather_right else nx - 1), chunks)

    parts = ys.at[pl.ds(0, 3)]

    def sum_send(s):
        if s in direct:
            for d in far_x:
                send(YX, ys.at[(x + d) % nx, s], ys_in.at[s, d - 1], yn_r.at[s], x_peer(d), parts)
            return
        on, off = (1, nx - 1) if s in sum_right else (nx - 1, 1)
        send(YX, ys.at[(x + 2) % nx, s], opp_in.at[s], yo_r.at[order.index(s)], x_peer(on), parts)
        send(YX, ys.at[(x + off) % nx, s], ys_in.at[s, 0], yn_r.at[s], x_peer(off), parts)

    def sum_pass(s):
        on = 1 if s in sum_right else nx - 1
        arrived(opp_in.at[s], yo_r.at[order.index(s)])
        opp_out[s] = (ys[(x + on) % nx, s].astype(F32) + opp_in[s].astype(F32)).astype(BF16)
        send(YX, opp_out.at[s], ys_in.at[s, 1], yn_r.at[s], x_peer(on), parts)

    def sum_end(s):
        count = nx - 1 if s in direct else 2
        arrived(ys_in.at[s, pl.ds(0, count)], yn_r.at[s])
        total = ys[x, s].astype(F32)
        for i in range(count):
            total = total + ys_in[s, i].astype(F32)
        if s == 0:
            ret[0] = total.astype(BF16)
        else:
            yy[s - 1] = total.astype(BF16)
            send(YG, yy.at[s - 1], ret.at[g_back(s)], in_r.at[YG], g_peer(s), yy)

    def experts(*ready):
        some = sum(ready, [])
        square = gated = raised = 0.0
        for d in (0, 1, nx - 1, 2):
            if d in (1, 2):
                for pair in ready:
                    arrived(xs.at[0, pl.ds(0, 2)], last(pair[0]) if d == 2 else rest(pair[0]))
            q = (x + d) % nx
            at = pl.ds(pl.multiple_of(q * quarter, quarter), quarter)
            piece = jnp.concatenate([xs[q, s].astype(F32) for s in some], axis=0)
            square = square + jnp.sum(piece * piece, axis=-1, keepdims=True)
            feats = (piece * fgain_v[:, at]).astype(BF16)
            gated = gated + mm(feats, eg_v[at, :])
            raised = raised + mm(feats, eu_v[at, :])
        scale = lax.rsqrt(square * (1.0 / width) + EPS)
        hidden = (silu(gated * scale) * (raised * scale)).astype(BF16)
        for i in range(nx):
            term = mm(hidden, ed_v[:, i * quarter : (i + 1) * quarter])
            for j, s in enumerate(some):
                ys[i, s] = term[j * part : (j + 1) * part].astype(BF16)
        for s in some:
            sum_send(s)

    local["fgain"].wait()
    local["gv"].wait()
    gain = [fgain_v[:, i * quarter : (i + 1) * quarter] for i in range(nx)]
    for name in ("eg", "eu", "ed"):
        local[name].wait()

    local["sg"].wait()
    local["su"].wait()
    columns = sgu_v.at[:, pl.ds(0, nz - 1), 0, 0]
    own = sgu_v.at[:, z, y, c]
    for d in far_z:
        send(SZ, own, own, in_r.at[SZ], z_peer(d), columns)

    gather_send(0)
    arrived(xs.at[x, 1], sl_r.at[1])
    gather_send(1)
    gather_pass(0)
    for at, s in enumerate(order[2:]):
        arrived(xs.at[x, s], sl_r.at[s])
        gather_send(s)
        if at == 1:
            gather_pass(1)
    for s in pairs[1]:
        gather_pass(s)
    experts(pairs[0])
    arrived(columns, in_r.at[SZ])
    three = sgu_v.at[:, :, pl.ds(0, 3), 0]
    near = sgu_v.at[:, :, y, c]
    for d in (1, ny - 1):
        send(SY, near, near, in_r.at[SY], g_peer(2 * d), three)
    for s in order[4:]:
        gather_pass(s)
    experts(pairs[1])
    for s in pairs[0]:
        sum_pass(s)
    experts(*pairs[2:])
    arrived(sgu_v.at[:, :, pl.ds(0, 2), 0], in_r.at[SY])
    mid = nz // 2
    low_half = sgu_v.at[:, pl.ds(0, mid), (y + ny - 1) % ny, c]
    high_half = sgu_v.at[:, pl.ds(mid, mid), (y + 1) % ny, c]
    send(SY, low_half, low_half, in_r.at[SC], g_peer(2), three)
    send(SY, high_half, high_half, in_r.at[SC], g_peer(2 * (ny - 1)), three)
    for s in order[2:]:
        if s not in direct:
            sum_pass(s)

    for s in order[:4] + direct:
        sum_end(s)
    arrived(near, in_r.at[SC])
    half = sgu_v.at[:, :, :, c]
    send(SC, half, half, in_r.at[SH], g_peer(1), sgu_v.at[:, :, :, 0])
    for s in order[4:]:
        if s not in direct:
            sum_end(s)

    arrived(att_in, in_r.at[RX])
    mine = [res16[i].astype(F32) for i in range(nx)]
    square = sum(jnp.sum(m * m, axis=-1, keepdims=True) for m in mine)
    scale = lax.rsqrt(square * (1.0 / width) + EPS)
    mix = [(mine[i] * scale * gain[i]).astype(BF16) for i in range(nx)]
    joined = jnp.concatenate(mix, axis=1)
    gv = gv_v[...].astype(F32)
    mix_gate = sum(
        joined[:, i * 128 : (i + 1) * 128].astype(F32) * gv[i : i + 1] for i in range(width // 128)
    )
    mix_gate = jnp.sum(mix_gate, axis=-1, keepdims=True)
    mix_gate = 1.0 / (1.0 + jnp.exp(-mix_gate))
    arrived(half, in_r.at[SH])
    local["sd"].wait()
    s_width = sgu_v.shape[-1]
    s_gate = mm(joined, sgu_v[0].reshape(width, s_width))
    s_up = mm(joined, sgu_v[1].reshape(width, s_width))
    s_hidden = (silu(s_gate) * s_up).astype(BF16)
    for i in range(nx):
        sh_out[i] = mm(s_hidden, sd_v[:, i * quarter : (i + 1) * quarter]).astype(BF16)
    for d in far_x:
        send(SH, sh_out.at[(x + d) % nx], sh_in.at[d - 1], in_r.at[ZB], x_peer(d), sh_in)

    arrived(ret.at[pl.ds(1, groups - 1)], in_r.at[YG])
    home = jnp.concatenate([ret[g].astype(F32) for g in range(groups)], axis=0).astype(BF16)
    routed = mm(comb[0][:, 0:slots], home) + mm(comb[1][:, 0:slots], home)
    for d in far_z:
        zs[d - 1] = routed[d * rows : (d + 1) * rows].astype(BF16)
        send(ZB, zs.at[d - 1], zs_in.at[d - 1], in_r.at[LAST], z_peer(d), zs)

    arrived(sh_in, in_r.at[ZB])
    shared = sh_out[x].astype(F32)
    for d in range(1, nx):
        shared = shared + sh_in[d - 1].astype(F32)
    final = res_v[...] + mix_gate * shared + routed[0:rows]
    arrived(zs_in, in_r.at[LAST])
    for d in range(1, nz):
        final = final + zs_in[d - 1].astype(F32)
    layer_out[...] = final.astype(BF16)
    for step, total in posted.items():
        arrived(total, out_s.at[step])


def shards(nz, ny, *args):
    (
        tokens,
        lengths,
        cache,
        attn_gain,
        query_weight,
        key_weight,
        value_weight,
        stick_bias,
        out_weight,
        ffn_gain,
        routes,
        route_weights,
        expert_gate,
        expert_up,
        expert_down,
        shared_gate,
        shared_up,
        shared_down,
        gate_vector,
    ) = args
    nx = lax.axis_size("tp")
    rows, width = tokens.shape
    quarter = width // nx
    groups = 2 * ny
    part = CAP * nz
    slots = groups * part
    lanes = -(-slots // 128) * 128
    heads = query_weight.shape[1] // HEAD_DIM
    length = cache.shape[1]
    vm = pltpu.VMEM
    dma = pltpu.SemaphoreType.DMA

    def like(a):
        return vm(a.shape, a.dtype)

    key_weight, value_weight = key_weight.T, value_weight.T
    routes, route_weights = routes.T, route_weights.T
    attn_gain = attn_gain.reshape(1, width)
    ffn_gain = ffn_gain.reshape(1, width)
    gate_vector = gate_vector.reshape(width // 128, 128)
    scratch = [
        pltpu.SMEM(lengths.shape, lengths.dtype),
        pltpu.SMEM(stick_bias.shape, stick_bias.dtype),
        like(tokens),
        vm((rows, quarter), BF16),
        like(attn_gain),
        like(ffn_gain),
        like(gate_vector),
        like(routes),
        like(route_weights),
        like(query_weight),
        like(key_weight),
        like(value_weight),
        like(out_weight),
        vm(expert_gate.shape[1:], BF16),
        vm(expert_up.shape[1:], BF16),
        vm(expert_down.shape[1:], BF16),
        like(shared_down),
        like(cache),
        vm((2, nz, ny, 2, *shared_gate.shape), BF16),
        vm((rows * heads, 2 * HEAD_DIM), F32),
        vm((rows * heads, 128), jnp.int32),
        vm((rows * heads, length), F32),
        vm((rows * heads, 2 * HEAD_DIM), F32),
        vm((nz, 8, 128), F32),
        vm((lanes, nz * rows), BF16),
        vm((2, nz * rows, lanes), BF16),
        vm((nx, rows, quarter), BF16),
        vm((nx - 1, rows, quarter), BF16),
        vm((rows, quarter), F32),
        vm((nx, rows, quarter), BF16),
        vm((nz, rows, quarter), BF16),
        vm((groups - 1, part, quarter), BF16),
        vm((nx, groups, part, quarter), BF16),
        vm((nx, groups, part, quarter), BF16),
        vm((groups, 3, part, quarter), BF16),
        vm((groups, part, quarter), BF16),
        vm((groups, part, quarter), BF16),
        vm((groups - 1, part, quarter), BF16),
        vm((groups, part, quarter), BF16),
        vm((nz - 1, rows, quarter), BF16),
        vm((nz - 1, rows, quarter), BF16),
        vm((nx, rows, quarter), BF16),
        vm((nx - 1, rows, quarter), BF16),
        dma((22,)),
        dma((4,)),
    ]
    scratch += [dma((13,)), dma((13,))] + [dma((n,)) for n in (groups, groups, groups - 2 * SUM_DIRECT, groups, groups)]
    spaces = [pltpu.HBM] * 19
    operands = (
        tokens,
        lengths,
        cache,
        attn_gain,
        query_weight,
        key_weight,
        value_weight,
        stick_bias,
        out_weight,
        ffn_gain,
        routes,
        route_weights,
        expert_gate,
        expert_up,
        expert_down,
        shared_gate,
        shared_up,
        shared_down,
        gate_vector,
    )
    return pl.pallas_call(
        functools.partial(kernel, (nz, ny, nx)),
        out_shape=(
            jax.ShapeDtypeStruct((rows, quarter), BF16),
            jax.ShapeDtypeStruct((rows, 2 * HEAD_DIM), BF16),
        ),
        in_specs=[pl.BlockSpec(memory_space=s) for s in spaces],
        out_specs=(
            pl.BlockSpec(memory_space=pltpu.VMEM),
            pl.BlockSpec(memory_space=pltpu.VMEM),
        ),
        scratch_shapes=scratch,
        compiler_params=pltpu.CompilerParams(
            collective_id=0, has_side_effects=True, vmem_limit_bytes=48 * 1024 * 1024
        ),
    )(*[pltpu.with_memory_space_constraint(a, pltpu.HBM) for a in operands])


def solution(mesh, ny=NY):
    nz = mesh.shape["ep"] // (2 * ny)
    placed = (
        P("ep", None),
        P("ep"),
        P("ep", None, "tp"),
        P(),
        P(None, "tp"),
        P(None, "tp"),
        P(None, "tp"),
        P("tp"),
        P("tp", None),
        P(),
        P("ep", None),
        P("ep", None),
        P("ep", None, "tp"),
        P("ep", None, "tp"),
        P("ep", "tp", None),
        P("ep", "tp"),
        P("ep", "tp"),
        P("tp", None),
        P(),
    )
    return jax.shard_map(
        functools.partial(shards, nz, ny),
        mesh=mesh,
        in_specs=placed,
        out_specs=(P("ep", "tp"), P("ep", "tp")),
        check_vma=False,
    )
```
